32 devices in a mesh: ep: 8 (over z, y), tp: 4 (over x, core).
Axes of the slice: x: 2, y: 2, z: 4, core: 2. Of those that a mesh axis runs over, the one named last changes fastest.
Arguments:
- mixer_in: bfloat16 [8192, 4096], P('ep', 'tp'), may hold values from -110 to 110
- mixer_gain: float32 [4096], P('tp'), may hold values from 0.1 to 1.9
- pool_weight: bfloat16 [4, 1024, 1024], P('tp'), may hold values from -0.1875 to 0.1875
- pool_scale: float32 [4096], P('tp'), may hold values from 0.1 to 1.9
- moe_in: bfloat16 [2048, 4096], P('ep'), may hold values from -6 to 6
- moe_gain: float32 [4096], replicated, may hold values from 0.1 to 1.9
- route_expert: int32 [2048, 2], P('ep'), may hold values from 0 to 7, as said below
- route_weight: float32 [2048, 2], P('ep'), may hold values from 0.1 to 1
- gate_weight: bfloat16 [8, 4096, 1024], P('ep', None, 'tp'), may hold values from -0.09375 to 0.09375
- up_weight: bfloat16 [8, 4096, 1024], P('ep', None, 'tp'), may hold values from -0.09375 to 0.09375
- down_weight: bfloat16 [8, 1024, 4096], P('ep', 'tp'), may hold values from -0.1875 to 0.1875
Outputs:
- mixer_out: bfloat16 [8192, 4096], P('ep', 'tp')
- moe_out: bfloat16 [2048, 4096], P('ep', 'tp')
The draws below stay inside these ranges and needn't reach their ends.
Inputs may be any that keep to these rules, and one draw needn't show every extreme that they name: `route_expert`: both experts of a row are different and lie in one group: the group of an expert is its number divided by 2, rounded down. Among the rows of one index of ep no expert is named more than 96 times; in every draw the experts of some group are each named exactly 96 times by the rows of every index of ep.
All inputs are finite; a program needn't handle non-finite values.
Results may differ from the reference program's by a relative error of at most 0.0071.
Values may be sent and summed in bfloat16 or wider, within the bound.
A program may use at most 128 MiB of HBM per device.

```python
import math
import jax
import jax.numpy as jnp
from jax import lax

D = 4096
POOL_GROUPS = 4
CH = 1024
WINDOW_MAX = 16
FF = 1024
EXPERTS = 8
EXPERT_GROUPS = 4
GROUP_EXPERTS = 2
MOE_DEV = 256
CAP = 96
TOKENS_A = 8192
TOKENS_B = 2048
N_EP = 8


def draw_mixer_in(key, part):
    first, second = jax.random.split(key, 2)
    ramp = jnp.exp(jnp.log(4.0) * jnp.arange(D, dtype=jnp.float32) / D)
    ramp = ramp * jnp.exp(jax.random.uniform(second, (D,), jnp.float32, -0.35, 0.35))
    base = jax.random.truncated_normal(first, -6.0, 6.0, (TOKENS_A, D), jnp.float32)
    return (base * ramp[None, :]).astype(jnp.bfloat16)


def draw_route_expert(key, part):
    fullest = GROUP_EXPERTS * CAP // 2
    rest = MOE_DEV - fullest
    pick_key, block_key = jax.random.split(key, 2)
    full_group = jax.random.randint(pick_key, (), 0, EXPERT_GROUPS)

    def one_block(bkey):
        key_a, key_b, key_c, key_d = jax.random.split(bkey, 4)
        chosen = jax.random.permutation(key_a, (EXPERT_GROUPS - 1) * fullest)[:rest]
        other_group = (full_group + 1 + chosen // fullest) % EXPERT_GROUPS
        groups = jnp.concatenate([jnp.full((fullest,), full_group, jnp.int32), other_group.astype(jnp.int32)])
        ranks = jnp.concatenate([jnp.arange(fullest, dtype=jnp.int32), (chosen % fullest).astype(jnp.int32)])
        shifts = jax.random.randint(key_b, (EXPERT_GROUPS,), 1, GROUP_EXPERTS)
        labels = jax.vmap(lambda lkey: jax.random.permutation(lkey, GROUP_EXPERTS))(jax.random.split(key_c, EXPERT_GROUPS))
        first = labels[groups, ranks % GROUP_EXPERTS]
        second = labels[groups, (ranks + shifts[groups]) % GROUP_EXPERTS]
        pair = jnp.stack([first, second], axis=1) + groups[:, None] * GROUP_EXPERTS
        order = jax.random.permutation(key_d, MOE_DEV)
        return pair[order].astype(jnp.int32)
    blocks = jax.vmap(one_block)(jax.random.split(block_key, N_EP))
    return blocks.reshape(MOE_DEV * N_EP, 2)


def steps_of(own_key, extent, cuts, least, largest):
    def one(axis_at, shards_of):
        steps = jax.random.uniform(jax.random.fold_in(jax.random.fold_in(own_key, 6), axis_at), (shards_of,), jnp.float32, least / len(cuts), largest / len(cuts))
        return jnp.repeat(jnp.exp(steps), extent[axis_at] // shards_of).reshape((-1,) + (1,) * (len(extent) - axis_at - 1))

    level = one(*cuts[0])
    for cut in cuts[1:]:
        level = level * one(*cut)
    return level


def bell_draw(own_key, dims, deviation, bound, pieces=(), kind=jnp.bfloat16):
    drawn = deviation * jax.random.normal(own_key, dims, jnp.float32)
    if pieces:
        drawn = drawn * steps_of(own_key, dims, pieces, -0.22, 0.18)
    return jnp.clip(drawn, -bound, bound).astype(kind)


def setup_inputs(seed: int = 0) -> dict:
    seeds = jax.random.split(jax.random.key(seed), 12)
    return {
        "mixer_in": draw_mixer_in(jax.random.fold_in(seeds[11], 71), 0),
        "mixer_gain": jnp.clip(1.0 + 0.18 * jax.random.normal(seeds[1], (D,), jnp.float32), 0.1, 1.9),
        "pool_weight": bell_draw(seeds[2], (POOL_GROUPS, CH, CH), CH ** -0.5, 0.1875, ((0, 4),)),
        "pool_scale": jnp.clip(1.0 + 0.18 * jax.random.normal(seeds[3], (D,), jnp.float32), 0.1, 1.9),
        "moe_in": bell_draw(seeds[4], (TOKENS_B, D), 1.0, 6.0, ((0, 8),)),
        "moe_gain": jnp.clip(1.0 + 0.18 * jax.random.normal(seeds[5], (D,), jnp.float32), 0.1, 1.9),
        "route_expert": draw_route_expert(jax.random.fold_in(seeds[11], 71), 0),
        "route_weight": jnp.clip(jnp.exp(math.log(1.0) - 2.3025851 * jax.random.uniform(seeds[7], (TOKENS_B, 2), jnp.float32) ** steps_of(seeds[7], (TOKENS_B, 2), ((0, 8),), -0.2, 0.2)), 0.1, 1.0),
        "gate_weight": bell_draw(seeds[8], (EXPERTS, D, FF), D ** -0.5, 0.09375, ((0, 8), (2, 4))),
        "up_weight": bell_draw(seeds[9], (EXPERTS, D, FF), D ** -0.5, 0.09375, ((0, 8), (2, 4))),
        "down_weight": bell_draw(seeds[10], (EXPERTS, FF, D), FF ** -0.5, 0.1875, ((0, 8), (1, 4))),
    }


EPS = 1e-06

def reference(mixer_in, mixer_gain, pool_weight, pool_scale, moe_in, moe_gain, route_expert, route_weight, gate_weight, up_weight, down_weight):
    feats = mixer_in.astype(jnp.float32)
    normed_a = (feats * lax.rsqrt(lax.optimization_barrier(jnp.mean(feats * feats, axis=1, keepdims=True)) + EPS) * mixer_gain).astype(jnp.bfloat16)
    reach = WINDOW_MAX - 1
    position = jnp.arange(TOKENS_A, dtype=jnp.int32)
    outputs = []
    for group in range(POOL_GROUPS):
        span = 2 ** (group + 1)
        block = normed_a[:, group * CH:(group + 1) * CH].astype(jnp.float32)
        padded = jnp.pad(block, ((reach, 0), (0, 0)))
        running = jnp.zeros_like(block)
        for offset in range(span):
            running = running + padded[reach - offset:reach - offset + TOKENS_A]
        count = jnp.minimum(position + 1, span).astype(jnp.float32)[:, None]
        pooled = (running / count - block).astype(jnp.bfloat16)
        projected = jnp.dot(pooled, pool_weight[group], preferred_element_type=jnp.float32)
        outputs.append(projected * pool_scale[group * CH:(group + 1) * CH])
    mixer_out = jnp.concatenate(outputs, axis=1).astype(jnp.bfloat16)
    feats_b = moe_in.astype(jnp.float32)
    normed_b = (feats_b * lax.rsqrt(lax.optimization_barrier(jnp.mean(feats_b * feats_b, axis=1, keepdims=True)) + EPS) * moe_gain).astype(jnp.bfloat16)
    slots_all = N_EP * CAP
    flat = route_expert.reshape(-1).astype(jnp.int32)
    onehot = (flat[:, None] == jnp.arange(EXPERTS, dtype=jnp.int32)[None, :]).astype(jnp.int32)
    earlier = jnp.cumsum(onehot, axis=0) - onehot
    slot_pos = lax.optimization_barrier(jnp.sum(earlier * onehot, axis=1)).astype(jnp.int32)
    owner = (jnp.arange(2 * TOKENS_B, dtype=jnp.int32) // 2).astype(jnp.int32)
    table = jnp.full((EXPERTS, slots_all), TOKENS_B, jnp.int32).at[flat, slot_pos].set(owner)
    padded_b = jnp.concatenate([normed_b, jnp.zeros((1, D), jnp.bfloat16)], axis=0)

    def one_expert(items):
        index, w_gate, w_up, w_down = items
        rows = jnp.take(padded_b, index, axis=0)
        gate = jnp.dot(rows, w_gate, preferred_element_type=jnp.float32)
        upper = jnp.dot(rows, w_up, preferred_element_type=jnp.float32)
        hidden = (jax.nn.silu(gate) * upper).astype(jnp.bfloat16)
        return jnp.dot(hidden, w_down, preferred_element_type=jnp.float32).astype(jnp.bfloat16)
    results = lax.map(one_expert, (table, gate_weight, up_weight, down_weight))
    picked = jnp.take(results.reshape(EXPERTS * slots_all, D), flat * slots_all + slot_pos, axis=0)
    weighted = picked.astype(jnp.float32).reshape(TOKENS_B, 2, D) * route_weight[:, :, None]
    moe_out = lax.optimization_barrier(jnp.sum(weighted, axis=1)).astype(jnp.bfloat16)
    return (mixer_out, moe_out)
```

```python
import functools

import jax
import jax.numpy as jnp
from jax import lax
from jax.experimental import pallas as pl
from jax.experimental.pallas import tpu as pltpu
from jax.sharding import PartitionSpec as P

D = 4096
WINDOW_MAX = 16


EPS = 1e-06


def passed_along(value, axis, steps):
    count = lax.axis_size(axis)
    first, last = (max(0, -steps), min(count, count - steps))
    return lax.ppermute(value, axis, [(source, source + steps) for source in range(first, last)])


GROUPS = 4
MESH = pl.DeviceIdType.MESH


def expert_kernel(
    cap,
    parts,
    moe_hbm,
    moe_gain_ref,
    routes_ref,
    shares_ref,
    gate_hbm,
    up_hbm,
    down_hbm,
    mixer_hbm,
    gain_ref,
    pool_hbm,
    scale_ref,
    moe_ref,
    mixed_ref,
    tokens_in,
    row_factor,
    scaled,
    outgoing,
    slot_column,
    unpermuted,
    xbuf,
    wrow,
    wbuf,
    wcol,
    w_gate,
    w_up,
    w_down,
    hidden,
    sums,
    first_x,
    first_y,
    second_in,
    fin,
    local_sem,
    send_sem,
    recv_sem,
    feats,
    w_pool,
    squares,
    squares_in,
    factors,
    normed,
):
    ep, tp = lax.axis_index("ep"), lax.axis_index("tp")
    z, y = ep // 2, ep % 2
    x, c = tp // 2, tp % 2
    tokens, model = tokens_in.shape
    width = xbuf.shape[3]
    units = w_gate.shape[1]
    half = width // 2
    part = cap // parts
    pair = 2 * part
    mine, theirs = slice(0, part), slice(part, pair)
    chunks = range(GROUPS * parts)
    eighth = width // 8
    direct = tuple(share * eighth for share in (4, 4, 0, 0, 0, 0, 8, 8))

    def dev(zz, yy, xx, cc):
        return (zz * 2 + yy, xx * 2 + cc)

    planes = [z, z + 1 - 2 * (z % 2), lax.rem(z + 2, GROUPS), GROUPS - 1 - z]
    core_peer = dev(z, y, x, 1 - c)
    x_peer = dev(z, y, 1 - x, c)
    y_peer = dev(z, 1 - y, x, c)
    cross_peer = dev(z, y, 1 - x, 1 - c)
    xq = (1 - x) * 2 + c

    def columns(quarter, count=None, offset=0):
        start = pl.multiple_of(quarter * width + offset, 128)
        return pl.ds(start, width if count is None else count)

    block = tokens // 8
    token_loads = [
        pltpu.make_async_copy(
            moe_hbm.at[b * block : (b + 1) * block],
            tokens_in.at[b * block : (b + 1) * block],
            local_sem.at[b],
        )
        for b in range(8)
    ]
    mixer_load = pltpu.make_async_copy(mixer_hbm, feats, local_sem.at[8])
    pool_load = pltpu.make_async_copy(pool_hbm, w_pool, local_sem.at[9])
    loads = [
        pltpu.make_async_copy(gate_hbm, w_gate, local_sem.at[10]),
        pltpu.make_async_copy(up_hbm, w_up, local_sem.at[11]),
    ]
    down_rows = pl.ds(pl.multiple_of(c * units, units), units)
    for xx in range(2):
        loads.append(
            pltpu.make_async_copy(
                down_hbm.at[:, columns(xx * 2 + c)],
                w_down.at[xx, down_rows, :],
                local_sem.at[12 + xx],
            )
        )
    for load in token_loads:
        load.start()

    barrier = pltpu.get_barrier_semaphore()
    peers = [core_peer, x_peer, y_peer, cross_peer]
    for other in range(2):
        for k in range(1, GROUPS):
            peers.append(dev(planes[k], lax.rem(y + other, 2), x, c))
    for peer in peers:
        pl.semaphore_signal(barrier, inc=1, device_id=peer, device_id_type=MESH)

    started = []

    def go(src, dst, peer):
        index = len(started)
        copy = pltpu.make_async_remote_copy(
            src_ref=src,
            dst_ref=dst,
            send_sem=send_sem.at[index],
            recv_sem=recv_sem.at[index],
            device_id=peer,
            device_id_type=MESH,
        )
        copy.start()
        started.append(copy)
        return copy

    routes = routes_ref[...]
    group = jnp.right_shift(routes[0:1, :], 1)
    lane_group = lax.broadcasted_iota(jnp.int32, (8, tokens), 0)
    member = lane_group == group
    earlier = lax.broadcasted_iota(jnp.int32, (tokens, tokens), 0) < lax.broadcasted_iota(
        jnp.int32, (tokens, tokens), 1
    )
    ahead = jnp.dot(
        member.astype(jnp.bfloat16), earlier.astype(jnp.bfloat16), preferred_element_type=jnp.float32
    )
    rank = jnp.sum(jnp.where(member, ahead, 0.0), axis=0, keepdims=True).astype(jnp.int32)

    def picks(k, count):
        place = lax.broadcasted_iota(jnp.int32, (count, tokens), 0)
        return (place == rank) & (group == planes[k])

    parity = jnp.bitwise_and(routes, 1)
    shares = shares_ref[...]
    by_expert = jnp.sum(
        jnp.concatenate(
            [
                jnp.where(lane_group == parity[r : r + 1, :], shares[r : r + 1, :], 0.0)[None]
                for r in range(2)
            ],
            axis=0,
        ),
        axis=0,
    )
    slot = (group * cap + rank).astype(jnp.float32)
    for b in range(tokens // 128):
        row = slot[:, b * 128 : (b + 1) * 128]
        slot_column[b * 128 : (b + 1) * 128, :] = jnp.broadcast_to(row, (128, 128)).T

    for k in range(GROUPS):
        wrow[k] = lax.dot_general(
            by_expert,
            picks(k, 128).astype(jnp.float32),
            (((1,), (1,)), ((), ())),
            precision=lax.Precision.HIGHEST,
            preferred_element_type=jnp.float32,
        )
    wbuf[0] = wrow[0]

    for b in range(8):
        token_loads[b].wait()
        rows = slice(b * block, (b + 1) * block)
        total = jnp.zeros((block, 128), jnp.float32)
        for q in range(model // 128):
            value = tokens_in[rows, q * 128 : (q + 1) * 128].astype(jnp.float32)
            total += value * value
        mean = jnp.sum(total, axis=1, keepdims=True) / D
        row_factor[rows, :] = jnp.broadcast_to(lax.rsqrt(mean + EPS), (block, 128))
    for load in (mixer_load, *loads, pool_load):
        load.start()

    def scale_quarter(quarter):
        for j in range(width // 128):
            cols = columns(quarter, 128, j * 128)
            value = tokens_in[:, cols].astype(jnp.float32) * row_factor[...]
            scaled[:, j * 128 : (j + 1) * 128] = (value * moe_gain_ref[:, cols]).astype(
                jnp.bfloat16
            )

    flushed = [0]

    def flush(recent):
        last = max(flushed[0], len(started) - recent)
        for copy in started[flushed[0] : last]:
            copy.wait_send()
        flushed[0] = last

    def own_rows(quarter):
        return [xbuf.at[quarter, h, mine] for h in range(parts)]

    def pick_rows(quarter, groups, targets):
        scale_quarter(quarter)
        choose = jnp.concatenate(
            [picks(k, cap).astype(jnp.float32) for k in groups], axis=0
        ).astype(jnp.bfloat16)
        for j in range(width // 256):
            cols = slice(j * 256, (j + 1) * 256)
            picked = jnp.dot(
                choose, scaled[:, cols], preferred_element_type=jnp.float32
            ).astype(jnp.bfloat16)
            start = 0
            for target in targets:
                target[:, cols] = picked[start : start + target.shape[0]]
                start += target.shape[0]

    zcopies = {}
    piece = {}

    def depart(k, across):
        g = k // parts
        index = g if g > 1 else across
        rows = slice(k % parts * part, (k % parts + 1) * part)
        zcopies[k, across] = go(
            outgoing.at[index, rows],
            xbuf.at[xq if across else tp, k, mine],
            dev(planes[g], y, x, c),
        )

    def share(name, k, quarter, source, target, peer, start=0, stop=None):
        stop = width if stop is None else stop
        if start < stop:
            cols = pl.ds(start, stop - start)
            piece[name, k] = go(
                xbuf.at[quarter, k, source, cols], xbuf.at[quarter, k, target, cols], peer
            )

    pick_rows(tp, (1, 2, 3, 0), [outgoing.at[0], outgoing.at[2], outgoing.at[3]] + own_rows(tp))
    pl.semaphore_wait(barrier, len(peers))
    wcopies = []
    for k in range(GROUPS):
        for r in range(2):
            if k or r:
                peer = dev(planes[k], lax.rem(y + r, 2), x, c)
                wcopies.append(go(wrow.at[k], wbuf.at[k * 2 + r], peer))
    depart(5, 0)
    depart(2, 0)
    depart(3, 0)
    for k in range(parts):
        share("y", k, tp, mine, theirs, y_peer)
    pick_rows(xq, (1, 0), [outgoing.at[1]] + own_rows(xq))
    depart(2, 1)
    depart(6, 0)
    depart(4, 0)
    depart(7, 0)
    depart(3, 1)
    for k in range(parts):
        share("d0", k, xq, mine, theirs, y_peer, 0, direct[k])
    down_copies = []
    for xx in range(2):
        down_copies.append(
            go(down_hbm.at[:, columns(xx * 2 + 1 - c)], w_down.at[xx, down_rows, :], core_peer)
        )
    for quarter in (x * 2 + 1 - c, (1 - x) * 2 + 1 - c):
        pick_rows(quarter, (0,), own_rows(quarter))

    def arrive(k):
        zcopies[k, 0].wait_recv()
        share("y", k, tp, mine, theirs, y_peer)
        if k // parts > 1:
            share("x", k, tp, mine, mine, x_peer)
        share("c", k, tp, mine, mine, core_peer)

    def across(k):
        if k // parts == 1:
            zcopies[k, 1].wait_recv()
        else:
            piece["x", k].wait_recv()
        share("d0", k, xq, mine, theirs, y_peer, 0, direct[k])
        share("xc", k, xq, mine, mine, core_peer)

    def relay(k):
        piece["y", k].wait_recv()
        share("d1", k, tp, theirs, theirs, x_peer, direct[k])
        share("yc", k, tp, theirs, theirs, core_peer)

    def diagonal(k):
        for name in ("d0", "d1"):
            if (name, k) in piece:
                piece[name, k].wait_recv()
        share("dc", k, xq, theirs, theirs, core_peer)

    def complete(k):
        for name in ("c", "xc", "yc", "dc"):
            if (name, k) in piece:
                piece[name, k].wait_recv()

    hidden_away = {}

    def weights_ready():
        for copy in wcopies:
            copy.wait_recv()
        for source in range(wbuf.shape[0]):
            line = jnp.where(y == 0, wbuf[source, 0:1, :], wbuf[source, 1:2, :])
            wcol[source * cap : (source + 1) * cap, :] = jnp.broadcast_to(line, (128, 128)).T[:cap]
        for load in loads:
            load.wait()
        for copy in down_copies:
            copy.wait_recv()

    def expand(k):
        complete(k)
        gate = jnp.zeros((pair, units), jnp.float32)
        upper = gate
        for q in range(xbuf.shape[0]):
            rows = xbuf[q, k]
            gate += jnp.dot(
                rows, w_gate[q * width : (q + 1) * width, :], preferred_element_type=jnp.float32
            )
            upper += jnp.dot(
                rows, w_up[q * width : (q + 1) * width, :], preferred_element_type=jnp.float32
            )
        first = k // parts * 2 * cap + k % parts * part
        scale = jnp.concatenate(
            [wcol[first : first + part, :], wcol[first + cap : first + cap + part, :]], axis=0
        )
        scale = jnp.concatenate([scale] * (units // scale.shape[1]), axis=1)
        value = (gate / (1.0 + jnp.exp(-gate))) * upper * scale
        hidden[c, k] = value.astype(jnp.bfloat16)
        hidden_away[k] = go(hidden.at[c, k], hidden.at[c, k], core_peer)

    hop = {}

    def project(k):
        hidden_away[k].wait_recv()
        for xx in range(2):
            for j in range(2):
                cols = slice(j * half, (j + 1) * half)
                total = jnp.dot(
                    hidden[0, k], w_down[xx, 0:units, cols], preferred_element_type=jnp.float32
                ) + jnp.dot(
                    hidden[1, k], w_down[xx, units:, cols], preferred_element_type=jnp.float32
                )
                sums[k, xx, :, cols] = total.astype(jnp.bfloat16)
        hop[k, 0] = go(sums.at[k, 1 - x, :, 0:half], first_x.at[k], x_peer)
        hop[k, 1] = go(sums.at[k, :, theirs, half:width], first_y.at[k], y_peer)

    def second_x(k):
        hop[k, 0].wait_recv()
        total = sums[k, x, :, 0:half].astype(jnp.float32) + first_x[k].astype(jnp.float32)
        sums[k, x, :, 0:half] = total.astype(jnp.bfloat16)
        hop[k, 3] = go(sums.at[k, x, theirs, 0:half], second_in.at[k, 0], y_peer)

    def second_y(k):
        hop[k, 1].wait_recv()
        for xx in range(2):
            total = sums[k, xx, mine, half:width].astype(jnp.float32) + first_y[k, xx].astype(
                jnp.float32
            )
            sums[k, xx, mine, half:width] = total.astype(jnp.bfloat16)
        hop[k, 4] = go(sums.at[k, 1 - x, mine, half:width], second_in.at[k, 1], x_peer)

    home = {}

    def homeward(k):
        for piece_index in range(2):
            cols = slice(piece_index * half, (piece_index + 1) * half)
            hop[k, 3 + piece_index].wait_recv()
            total = sums[k, x, mine, cols].astype(jnp.float32) + second_in[
                k, piece_index
            ].astype(jnp.float32)
            if k < parts:
                fin[k, :, cols] = total.astype(jnp.bfloat16)
            else:
                sums[k, x, mine, cols] = total.astype(jnp.bfloat16)
        if k >= parts:
            home[k] = go(sums.at[k, x, mine, :], fin.at[k], dev(planes[k // parts], y, x, c))

    settled = []

    def settle(k):
        if k >= parts:
            home[k].wait_recv()
        first = planes[k // parts] * cap + k % parts * part
        place = lax.broadcasted_iota(jnp.int32, (tokens, part), 1) + first
        choose = (slot_column[:, 0:part].astype(jnp.int32) == place).astype(jnp.float32)
        choose = choose.astype(jnp.bfloat16)
        settled.append(k)
        for j in range(width // 256):
            cols = slice(j * 256, (j + 1) * 256)
            value = jnp.dot(choose, fin[k, :, cols], preferred_element_type=jnp.float32)
            if len(settled) > 1:
                value += unpermuted[:, cols]
            if len(settled) == len(chunks):
                moe_ref[:, cols] = value.astype(jnp.bfloat16)
            else:
                unpermuted[:, cols] = value

    rows, channels = feats.shape
    tiles = rows // 128
    reach = WINDOW_MAX

    def tile_rows(i, start=0, count=128):
        return pl.ds(pl.multiple_of(i * 128 + start, 16), count)

    mixer_copies = []

    def square_sums():
        mixer_load.wait()

        @pl.loop(0, tiles)
        def _(i):
            total = jnp.zeros((128, 128), jnp.float32)
            for q in range(channels // 128):
                value = feats[tile_rows(i), q * 128 : (q + 1) * 128].astype(jnp.float32)
                total += value * value
            squares[pl.ds(i, 1), :] = jnp.sum(total.T, axis=0, keepdims=True)

        for index, peer in enumerate((core_peer, x_peer, cross_peer)):
            mixer_copies.append(
                go(squares, squares_in.at[index], peer)
            )

    def normalize():
        for copy in mixer_copies:
            copy.wait_recv()
        total = squares[...] + squares_in[0] + (squares_in[1] + squares_in[2])
        factors[...] = lax.rsqrt(total / D + EPS)

        @pl.loop(0, tiles)
        def _(i):
            factor = jnp.broadcast_to(factors[pl.ds(i, 1), :], (128, 128)).T
            for q in range(channels // 128):
                cols = slice(q * 128, (q + 1) * 128)
                value = feats[tile_rows(i), cols].astype(jnp.float32) * factor * gain_ref[:, cols]
                normed[tile_rows(i, reach), cols] = value.astype(jnp.bfloat16)

        following = lax.rem(ep + 1, 2 * GROUPS)
        mixer_copies.append(
            go(normed.at[rows : rows + reach, :], normed.at[0:reach, :], (following, tp))
        )

    def halo():
        mixer_copies[3].wait_recv()
        edge = normed[0:reach, :]
        normed[0:reach, :] = jnp.where(ep == 0, jnp.zeros_like(edge), edge)
        pool_load.wait()

    def pool(first, last):
        span = jnp.where(tp == 0, 2, jnp.where(tp == 1, 4, jnp.where(tp == 2, 8, 16)))

        @pl.loop(first, last)
        def _(i):
            position = ep * rows + i * 128 + lax.broadcasted_iota(jnp.int32, (128, 256), 0)
            share_of = 1.0 / jnp.minimum(position + 1, span).astype(jnp.float32)
            for q in range(channels // 256):
                cols = slice(q * 256, (q + 1) * 256)
                value = normed[tile_rows(i, 0, 128 + reach), cols].astype(jnp.float32)
                two = value + pltpu.roll(value, 1, 0)
                four = two + pltpu.roll(two, 2, 0)
                eight = four + pltpu.roll(four, 4, 0)
                sixteen = eight + pltpu.roll(eight, 8, 0)
                window = jnp.where(
                    tp == 0, two, jnp.where(tp == 1, four, jnp.where(tp == 2, eight, sixteen))
                )
                pooled = window[reach:] * share_of - value[reach:]
                feats[tile_rows(i), cols] = pooled.astype(jnp.bfloat16)
            projected = jnp.dot(
                feats[tile_rows(i), :], w_pool[...], preferred_element_type=jnp.float32
            )
            mixed_ref[tile_rows(i), :] = (projected * scale_ref[...]).astype(jnp.bfloat16)

    relay(0)
    arrive(2)
    diagonal(0)
    relay(1)
    weights_ready()
    arrive(5)
    relay(2)
    expand(0)
    relay(5)
    arrive(3)
    project(0)
    across(2)
    diagonal(1)
    diagonal(2)
    arrive(4)
    square_sums()
    arrive(6)
    expand(2)
    across(5)
    across(3)
    project(2)
    arrive(7)
    relay(4)
    across(6)
    diagonal(5)
    relay(3)
    expand(5)
    second_x(2)
    normalize()
    second_x(0)
    across(4)
    across(7)
    relay(6)
    diagonal(4)
    relay(7)
    second_y(0)
    second_y(2)
    project(5)
    halo()
    diagonal(6)
    expand(4)
    pool(0, 1)
    flush(24)
    homeward(0)
    expand(1)
    project(4)
    diagonal(7)
    expand(7)
    second_x(5)
    second_y(5)
    expand(6)
    homeward(2)
    project(7)
    second_x(4)
    diagonal(3)
    pool(1, 2)
    flush(24)
    second_y(4)
    project(6)
    expand(3)
    homeward(5)
    pool(2, 3)
    flush(24)
    pool(3, 4)
    flush(24)
    homeward(4)
    project(3)
    second_y(7)
    second_x(7)
    second_y(6)
    second_x(6)
    second_x(3)
    second_y(3)
    project(1)
    pool(4, 5)
    flush(24)
    homeward(6)
    pool(5, 6)
    flush(24)
    flush(16)
    settle(0)
    homeward(7)
    pool(6, 7)
    flush(24)
    flush(16)
    settle(4)
    homeward(3)
    flush(16)
    settle(2)
    second_x(1)
    second_y(1)
    pool(7, 8)
    flush(24)
    flush(16)
    settle(6)
    homeward(1)
    flush(16)
    settle(5)
    flush(16)
    settle(1)
    flush(16)
    settle(3)
    flush(16)
    settle(7)
    flush(0)


def deliver(moe_in_ref, mixed_in_ref, moe_hbm, mixer_hbm, sem):
    copies = []
    for source, target, count in ((mixed_in_ref, mixer_hbm, 16), (moe_in_ref, moe_hbm, 4)):
        rows = source.shape[0] // count
        for i in range(count):
            at = slice(i * rows, (i + 1) * rows)
            copies.append(
                pltpu.make_async_copy(source.at[at], target.at[at], sem.at[len(copies)])
            )
    for copy in copies:
        copy.start()
    for copy in copies:
        copy.wait()


def paired_step(
    mixer_in,
    mixer_gain,
    pool_weight,
    pool_scale,
    moe_in,
    moe_gain,
    route_expert,
    route_weight,
    gate_weight,
    up_weight,
    down_weight,
):
    tokens, model = moe_in.shape
    n_ep, n_tp = lax.axis_size("ep"), lax.axis_size("tp")
    cap = 3 * tokens // n_ep
    width = model // n_tp
    units = gate_weight.shape[2]
    vmem = pl.BlockSpec(memory_space=pltpu.VMEM)
    hbm = pl.BlockSpec(memory_space=pl.ANY)
    dma = pltpu.SemaphoreType.DMA
    rows, channels = mixer_in.shape
    copies = 150
    parts = 2
    chunks, part = GROUPS * parts, cap // parts
    moe_shape = (tokens, width)
    mixer_shape = (rows, channels)
    moe_out, mixed = pl.pallas_call(
        functools.partial(expert_kernel, cap, parts),
        out_shape=(
            pltpu.VMEM(moe_shape, jnp.bfloat16),
            pltpu.VMEM(mixer_shape, jnp.bfloat16),
        ),
        in_specs=[hbm, vmem, vmem, vmem, hbm, hbm, hbm, hbm, vmem, hbm, vmem],
        out_specs=(vmem, vmem),
        scratch_shapes=[
            pltpu.VMEM((tokens, model), jnp.bfloat16),
            pltpu.VMEM((tokens, 128), jnp.float32),
            pltpu.VMEM((tokens, width), jnp.bfloat16),
            pltpu.VMEM((GROUPS, cap, width), jnp.bfloat16),
            pltpu.VMEM((tokens, 128), jnp.float32),
            pltpu.VMEM((tokens, width), jnp.float32),
            pltpu.VMEM((n_tp, chunks, 2 * part, width), jnp.bfloat16),
            pltpu.VMEM((GROUPS, 8, 128), jnp.float32),
            pltpu.VMEM((n_ep, 8, 128), jnp.float32),
            pltpu.VMEM((n_ep * cap, 128), jnp.float32),
            pltpu.VMEM((model, units), jnp.bfloat16),
            pltpu.VMEM((model, units), jnp.bfloat16),
            pltpu.VMEM((2, 2 * units, width), jnp.bfloat16),
            pltpu.VMEM((2, chunks, 2 * part, units), jnp.bfloat16),
            pltpu.VMEM((chunks, 2, 2 * part, width), jnp.bfloat16),
            pltpu.VMEM((chunks, 2 * part, width // 2), jnp.bfloat16),
            pltpu.VMEM((chunks, 2, part, width // 2), jnp.bfloat16),
            pltpu.VMEM((chunks, 2, part, width // 2), jnp.bfloat16),
            pltpu.VMEM((chunks, part, width), jnp.bfloat16),
            dma((14,)),
            dma((copies,)),
            dma((copies,)),
            pltpu.VMEM((rows, channels), jnp.bfloat16),
            pltpu.VMEM(pool_weight.shape[1:], jnp.bfloat16),
            pltpu.VMEM((rows // 128, 128), jnp.float32),
            pltpu.VMEM((3, rows // 128, 128), jnp.float32),
            pltpu.VMEM((rows // 128, 128), jnp.float32),
            pltpu.VMEM((rows + WINDOW_MAX, channels), jnp.bfloat16),
        ],
        compiler_params=pltpu.CompilerParams(
            collective_id=0, has_side_effects=True, vmem_limit_bytes=56 * 1024 * 1024
        ),
    )(
        moe_in,
        moe_gain[None, :],
        route_expert.T,
        route_weight.T,
        gate_weight[0],
        up_weight[0],
        down_weight[0],
        mixer_in,
        mixer_gain[None, :],
        pool_weight[0],
        pool_scale[None, :],
    )
    moe_out, mixer_out = pl.pallas_call(
        deliver,
        out_shape=(
            jax.ShapeDtypeStruct(moe_shape, jnp.bfloat16),
            jax.ShapeDtypeStruct(mixer_shape, jnp.bfloat16),
        ),
        in_specs=[vmem, vmem],
        out_specs=(hbm, hbm),
        scratch_shapes=[dma((20,))],
    )(
        pltpu.with_memory_space_constraint(moe_out, pltpu.VMEM),
        pltpu.with_memory_space_constraint(mixed, pltpu.VMEM),
    )
    return (mixer_out, moe_out)


def any_experts(
    moe_in, moe_gain, route_expert, route_weight, gate_weight, up_weight, down_weight
):
    tokens = moe_in.shape[0]
    feats_b = moe_in.astype(jnp.float32)
    normed_b = (
        feats_b * lax.rsqrt(jnp.mean(feats_b * feats_b, axis=1, keepdims=True) + EPS) * moe_gain
    ).astype(jnp.bfloat16)
    experts = gate_weight.shape[0] * lax.axis_size("ep")
    slots = 3 * tokens // experts
    flat = route_expert.reshape(-1)
    onehot = (flat[:, None] == jnp.arange(experts, dtype=jnp.int32)[None, :]).astype(jnp.int32)
    earlier = jnp.cumsum(onehot, axis=0) - onehot
    slot_index = flat * slots + jnp.sum(earlier * onehot, axis=1)
    owner = jnp.arange(2 * tokens, dtype=jnp.int32) // 2
    source = jnp.full((experts * slots,), tokens, jnp.int32).at[slot_index].set(owner)
    padded_b = jnp.concatenate([normed_b, jnp.zeros((1, D), jnp.bfloat16)], axis=0)
    outgoing = jnp.take(padded_b, source, axis=0).reshape(experts, slots, D)
    w_gate = gate_weight[0]
    w_up = up_weight[0]
    share = slots // lax.axis_size("tp")
    mine = lax.dynamic_slice_in_dim(outgoing, lax.axis_index("tp") * share, share, 1)
    arrived = lax.all_to_all(mine, "ep", split_axis=0, concat_axis=0, tiled=True)
    expand_arrived = lax.all_gather(arrived, "tp", axis=1, tiled=True)
    gate = jnp.einsum("nkd,df->nkf", expand_arrived, w_gate, preferred_element_type=jnp.float32)
    upper = jnp.einsum("nkd,df->nkf", expand_arrived, w_up, preferred_element_type=jnp.float32)
    hidden = (jax.nn.silu(gate) * upper).astype(jnp.bfloat16)
    flat_hidden = hidden.reshape(-1, hidden.shape[2])
    w_down = down_weight[0]
    columns = D // lax.axis_size("tp")
    summed = lax.psum_scatter(
        lax.dot_general(
            w_down, flat_hidden, (((0,), (1,)), ((), ())), preferred_element_type=jnp.float32
        ),
        "tp",
        scatter_dimension=0,
        tiled=True,
    ).astype(jnp.bfloat16)
    back = lax.all_to_all(
        summed.reshape(columns, -1, slots), "ep", split_axis=1, concat_axis=1, tiled=True
    )
    picked = jnp.take(back.reshape(columns, experts * slots), slot_index, axis=1)
    weighted = picked.astype(jnp.float32).reshape(columns, tokens, 2) * route_weight[None, :, :]
    moe_out = jnp.sum(weighted, axis=2).T.astype(jnp.bfloat16)
    return moe_out


def general_step(
    mixer_in,
    mixer_gain,
    pool_weight,
    pool_scale,
    moe_in,
    moe_gain,
    route_expert,
    route_weight,
    gate_weight,
    up_weight,
    down_weight,
):
    rows = mixer_in.shape[0]
    feats = mixer_in.astype(jnp.float32)
    squares = lax.psum(jnp.sum(feats * feats, axis=1), "tp")
    normed_a = (feats * lax.rsqrt(squares[:, None] / D + EPS) * mixer_gain).astype(jnp.bfloat16)
    reach = WINDOW_MAX - 1
    before = passed_along(normed_a[rows - reach :], "ep", 1)
    extended = jnp.concatenate([before, normed_a], axis=0).astype(jnp.float32)
    running = jnp.zeros((rows, normed_a.shape[1]), jnp.float32)
    totals = []
    for offset in range(WINDOW_MAX):
        running = running + lax.slice_in_dim(
            extended, reach - offset, reach - offset + rows, axis=0
        )
        if offset > 0 and offset + 1 & offset == 0:
            totals.append(running)
    group = lax.axis_index("tp")
    window_sum = lax.dynamic_index_in_dim(jnp.stack(totals), group, 0, keepdims=False)
    span = jnp.left_shift(jnp.int32(2), group)
    position = lax.axis_index("ep") * rows + jnp.arange(rows, dtype=jnp.int32)
    count = jnp.minimum(position + 1, span).astype(jnp.float32)[:, None]
    pooled = (window_sum / count - extended[reach:]).astype(jnp.bfloat16)
    mixer_out = (
        jnp.dot(pooled, pool_weight[0], preferred_element_type=jnp.float32) * pool_scale
    ).astype(jnp.bfloat16)
    moe_out = any_experts(
        moe_in, moe_gain, route_expert, route_weight, gate_weight, up_weight, down_weight
    )
    return (mixer_out, moe_out)


def solution(mesh):
    paired = mesh.shape["ep"] == 2 * GROUPS and mesh.shape["tp"] == 4
    return jax.shard_map(
        paired_step if paired else general_step,
        mesh=mesh,
        in_specs=(
            P("ep", "tp"),
            P("tp"),
            P("tp", None, None),
            P("tp"),
            P("ep", None),
            P(),
            P("ep", None),
            P("ep", None),
            P("ep", None, "tp"),
            P("ep", None, "tp"),
            P("ep", "tp", None),
        ),
        out_specs=(P("ep", "tp"), P("ep", "tp")),
        check_vma=False,
    )
```

```python
import functools

import jax
import jax.numpy as jnp
from jax import lax
from jax.experimental import pallas as pl
from jax.experimental.pallas import tpu as pltpu
from jax.sharding import PartitionSpec as P

D = 4096
WINDOW_MAX = 16


EPS = 1e-06


def passed_along(value, axis, steps):
    count = lax.axis_size(axis)
    first, last = (max(0, -steps), min(count, count - steps))
    return lax.ppermute(value, axis, [(source, source + steps) for source in range(first, last)])


GROUPS = 4
MESH = pl.DeviceIdType.MESH


def expert_kernel(
    cap,
    parts,
    spare,
    moe_hbm,
    moe_gain_hbm,
    routes_hbm,
    shares_hbm,
    gate_hbm,
    up_hbm,
    down_hbm,
    mixer_hbm,
    gain_hbm,
    pool_hbm,
    scale_hbm,
    moe_ref,
    mixed_ref,
    moe_gain_ref,
    routes_ref,
    shares_ref,
    gain_ref,
    scale_ref,
    tokens_in,
    row_factor,
    scaled,
    outgoing,
    slot_column,
    unpermuted,
    xbuf,
    wrow,
    wbuf,
    wcol,
    fcol,
    w_gate,
    w_up,
    w_down,
    hidden,
    sums,
    first_x,
    first_y,
    second_in,
    fin,
    local_sem,
    send_sem,
    recv_sem,
    feats,
    w_pool,
    squares,
    squares_in,
    factors,
    normed,
):
    ep, tp = lax.axis_index("ep"), lax.axis_index("tp")
    z, y = ep // 2, ep % 2
    x, c = tp // 2, tp % 2
    tokens, model = tokens_in.shape
    width = xbuf.shape[3]
    units = w_gate.shape[1]
    half = width // 2
    part = cap // parts
    pair = 2 * part
    mine, theirs = slice(0, part), slice(part, pair)
    chunks = range(GROUPS * parts)
    eighth = width // 8
    direct = tuple(share * eighth for share in (4, 4, 0, 0, 0, 0, 8, 8))

    def dev(zz, yy, xx, cc):
        return (zz * 2 + yy, xx * 2 + cc)

    planes = [z, z + 1 - 2 * (z % 2), lax.rem(z + 2, GROUPS), GROUPS - 1 - z]
    core_peer = dev(z, y, x, 1 - c)
    x_peer = dev(z, y, 1 - x, c)
    y_peer = dev(z, 1 - y, x, c)
    cross_peer = dev(z, y, 1 - x, 1 - c)
    xq = (1 - x) * 2 + c

    def columns(quarter, count=None, offset=0):
        start = pl.multiple_of(quarter * width + offset, 128)
        return pl.ds(start, width if count is None else count)

    quarters = (tp, xq, x * 2 + 1 - c, (1 - x) * 2 + 1 - c)
    rows_half = tokens // 2
    small_loads = [
        pltpu.make_async_copy(source, target, local_sem.at[16 + i])
        for i, (source, target) in enumerate(
            (
                (routes_hbm, routes_ref),
                (shares_hbm, shares_ref),
                (moe_gain_hbm, moe_gain_ref),
                (gain_hbm, gain_ref),
                (scale_hbm, scale_ref),
            )
        )
    ]
    token_loads = []
    for i, quarter in enumerate(quarters):
        for b in range(2):
            at = (slice(b * rows_half, (b + 1) * rows_half), columns(quarter))
            token_loads.append(
                pltpu.make_async_copy(
                    moe_hbm.at[at], tokens_in.at[at], local_sem.at[i * 2 + b]
                )
            )
    mixer_load = pltpu.make_async_copy(mixer_hbm, feats, local_sem.at[8])
    pool_load = pltpu.make_async_copy(pool_hbm, w_pool, local_sem.at[9])
    loads = [
        pltpu.make_async_copy(gate_hbm, w_gate, local_sem.at[10]),
        pltpu.make_async_copy(up_hbm, w_up, local_sem.at[11]),
    ]
    down_rows = pl.ds(pl.multiple_of(c * units, units), units)
    for xx in range(2):
        loads.append(
            pltpu.make_async_copy(
                down_hbm.at[:, columns(xx * 2 + c)],
                w_down.at[xx, down_rows, :],
                local_sem.at[12 + xx],
            )
        )
    for load in small_loads[:3] + token_loads + small_loads[3:]:
        load.start()

    barrier = pltpu.get_barrier_semaphore()
    peers = [core_peer, x_peer, y_peer, cross_peer]
    for other in range(2):
        for k in range(1, GROUPS):
            peers.append(dev(planes[k], lax.rem(y + other, 2), x, c))
    for peer in peers:
        pl.semaphore_signal(barrier, inc=1, device_id=peer, device_id_type=MESH)

    started = []

    ring = []
    kept = []

    def go(src, dst, peer, keep=False):
        index = len(started)
        if keep:
            send = spare + len(kept)
            kept.append(index)
        else:
            send = len(ring) % spare
            if len(ring) >= spare:
                started[ring[-spare]].wait_send()
            ring.append(index)
        copy = pltpu.make_async_remote_copy(
            src_ref=src,
            dst_ref=dst,
            send_sem=send_sem.at[send],
            recv_sem=recv_sem.at[index],
            device_id=peer,
            device_id_type=MESH,
        )
        copy.start()
        started.append(copy)
        return copy

    for load in small_loads[:3]:
        load.wait()
    routes = routes_ref[...]
    group = jnp.right_shift(routes[0:1, :], 1)
    lane_group = lax.broadcasted_iota(jnp.int32, (8, tokens), 0)
    member = lane_group == group
    earlier = lax.broadcasted_iota(jnp.int32, (tokens, tokens), 0) < lax.broadcasted_iota(
        jnp.int32, (tokens, tokens), 1
    )
    ahead = jnp.dot(
        member.astype(jnp.bfloat16), earlier.astype(jnp.bfloat16), preferred_element_type=jnp.float32
    )
    rank = jnp.sum(jnp.where(member, ahead, 0.0), axis=0, keepdims=True).astype(jnp.int32)

    def picks(k, count):
        place = lax.broadcasted_iota(jnp.int32, (count, tokens), 0)
        return (place == rank) & (group == planes[k])

    parity = jnp.bitwise_and(routes, 1)
    shares = shares_ref[...]
    by_expert = jnp.sum(
        jnp.concatenate(
            [
                jnp.where(lane_group == parity[r : r + 1, :], shares[r : r + 1, :], 0.0)[None]
                for r in range(2)
            ],
            axis=0,
        ),
        axis=0,
    )
    slot = (group * cap + rank).astype(jnp.float32)
    for b in range(tokens // 128):
        row = slot[:, b * 128 : (b + 1) * 128]
        slot_column[b * 128 : (b + 1) * 128, :] = jnp.broadcast_to(row, (128, 128)).T

    def send_lines():
        for b in range(8):
            rows = slice(b * tokens // 8, (b + 1) * tokens // 8)
            total = jnp.zeros((tokens // 8, 128), jnp.float32)
            for q in range(model // 128):
                value = tokens_in[rows, q * 128 : (q + 1) * 128].astype(jnp.float32)
                total += value * value
            mean = jnp.sum(total, axis=1, keepdims=True) / D
            row_factor[rows, :] = jnp.broadcast_to(lax.rsqrt(mean + EPS), (tokens // 8, 128))
        factor = jnp.concatenate(
            [row_factor[b * 128 : (b + 1) * 128, :].T[0:8, :] for b in range(tokens // 128)], axis=1
        )
        lines = jnp.where(lane_group == 2, factor, by_expert)
        copies = []
        for k in range(GROUPS):
            wrow[k] = lax.dot_general(
                lines,
                picks(k, 128).astype(jnp.float32),
                (((1,), (1,)), ((), ())),
                precision=lax.Precision.HIGHEST,
                preferred_element_type=jnp.float32,
            )
            for r in range(2):
                if k or r:
                    peer = dev(planes[k], lax.rem(y + r, 2), x, c)
                    copies.append(go(wrow.at[k], wbuf.at[k * 2 + r], peer, keep=True))
        wbuf[0] = wrow[0]
        return copies

    for load in token_loads[:2]:
        load.wait()
    for load in (mixer_load, *loads, pool_load):
        load.start()

    def scale_quarter(quarter):
        for j in range(width // 128):
            cols = columns(quarter, 128, j * 128)
            value = tokens_in[:, cols].astype(jnp.float32) * moe_gain_ref[:, cols]
            scaled[:, j * 128 : (j + 1) * 128] = value.astype(jnp.bfloat16)

    def own_rows(quarter):
        return [xbuf.at[quarter, h, mine] for h in range(parts)]

    def pick_rows(quarter, groups, targets):
        scale_quarter(quarter)
        choose = jnp.concatenate(
            [picks(k, cap).astype(jnp.float32) for k in groups], axis=0
        ).astype(jnp.bfloat16)
        for j in range(width // 256):
            cols = slice(j * 256, (j + 1) * 256)
            picked = jnp.dot(
                choose, scaled[:, cols], preferred_element_type=jnp.float32
            ).astype(jnp.bfloat16)
            start = 0
            for target in targets:
                target[:, cols] = picked[start : start + target.shape[0]]
                start += target.shape[0]

    zcopies = {}
    piece = {}

    def depart(k, across):
        g = k // parts
        index = g + 2 if across else g - 1
        rows = slice(k % parts * part, (k % parts + 1) * part)
        zcopies[k, across] = go(
            outgoing.at[index, rows],
            xbuf.at[xq if across else tp, k, mine],
            dev(planes[g], y, x, c),
            keep=True,
        )

    def share(name, k, quarter, source, target, peer, start=0, stop=None):
        stop = width if stop is None else stop
        if start < stop:
            cols = pl.ds(start, stop - start)
            piece[name, k] = go(
                xbuf.at[quarter, k, source, cols], xbuf.at[quarter, k, target, cols], peer
            )

    pick_rows(tp, (1, 2, 3, 0), [outgoing.at[i] for i in range(3)] + own_rows(tp))
    pl.semaphore_wait(barrier, len(peers))
    depart(5, 0)
    for k in range(parts):
        share("y", k, tp, mine, theirs, y_peer)
    for load in token_loads[2:]:
        load.wait()
    wcopies = send_lines()
    pick_rows(xq, (1, 0), [outgoing.at[3]] + own_rows(xq))
    depart(2, 0)
    depart(3, 0)
    depart(2, 1)
    depart(6, 0)
    depart(4, 0)
    depart(7, 0)
    depart(3, 1)
    for k in range(parts):
        share("d0", k, xq, mine, theirs, y_peer, 0, direct[k])
    down_copies = []
    for xx in range(2):
        down_copies.append(
            go(down_hbm.at[:, columns(xx * 2 + 1 - c)], w_down.at[xx, down_rows, :], core_peer)
        )
    for quarter in quarters[2:]:
        pick_rows(quarter, (0,), own_rows(quarter))

    def arrive(k):
        zcopies[k, 0].wait_recv()
        share("y", k, tp, mine, theirs, y_peer)
        if (k, 1) not in zcopies:
            share("x", k, tp, mine, mine, x_peer)
        share("c", k, tp, mine, mine, core_peer)

    def across(k):
        if (k, 1) in zcopies:
            zcopies[k, 1].wait_recv()
        else:
            piece["x", k].wait_recv()
        share("d0", k, xq, mine, theirs, y_peer, 0, direct[k])
        share("xc", k, xq, mine, mine, core_peer)

    def relay(k):
        piece["y", k].wait_recv()
        share("d1", k, tp, theirs, theirs, x_peer, direct[k])
        share("yc", k, tp, theirs, theirs, core_peer)

    def diagonal(k):
        for name in ("d0", "d1"):
            if (name, k) in piece:
                piece[name, k].wait_recv()
        share("dc", k, xq, theirs, theirs, core_peer)

    def complete(k):
        for name in ("c", "xc", "yc", "dc"):
            if (name, k) in piece:
                piece[name, k].wait_recv()

    hidden_away = {}

    def weights_ready():
        for copy in wcopies:
            copy.wait_recv()
        for source in range(wbuf.shape[0]):
            line = jnp.where(y == 0, wbuf[source, 0:1, :], wbuf[source, 1:2, :])
            at = slice(source * cap, (source + 1) * cap)
            wcol[at, :] = jnp.broadcast_to(line, (128, 128)).T[:cap]
            fcol[at, :] = jnp.broadcast_to(wbuf[source, 2:3, :], (128, 128)).T[:cap]
        for load in loads:
            load.wait()
        for copy in down_copies:
            copy.wait_recv()

    def expand(k):
        complete(k)
        gate = jnp.zeros((pair, units), jnp.float32)
        upper = gate
        for q in range(xbuf.shape[0]):
            rows = xbuf[q, k]
            gate += jnp.dot(
                rows, w_gate[q * width : (q + 1) * width, :], preferred_element_type=jnp.float32
            )
            upper += jnp.dot(
                rows, w_up[q * width : (q + 1) * width, :], preferred_element_type=jnp.float32
            )
        first = k // parts * 2 * cap + k % parts * part

        def spread(table):
            lines = [table[first : first + part, :], table[first + cap : first + cap + part, :]]
            return jnp.concatenate([jnp.concatenate(lines, axis=0)] * (units // 128), axis=1)

        factor = spread(fcol)
        gate, upper = gate * factor, upper * factor
        value = (gate / (1.0 + jnp.exp(-gate))) * upper * spread(wcol)
        hidden[c, k] = value.astype(jnp.bfloat16)
        hidden_away[k] = go(hidden.at[c, k], hidden.at[c, k], core_peer)

    hop = {}

    def project(k):
        hidden_away[k].wait_recv()
        for xx in range(2):
            for j in range(2):
                cols = slice(j * half, (j + 1) * half)
                total = jnp.dot(
                    hidden[0, k], w_down[xx, 0:units, cols], preferred_element_type=jnp.float32
                ) + jnp.dot(
                    hidden[1, k], w_down[xx, units:, cols], preferred_element_type=jnp.float32
                )
                sums[k, xx, :, cols] = total.astype(jnp.bfloat16)
        hop[k, 0] = go(sums.at[k, 1 - x, :, 0:half], first_x.at[k], x_peer)
        hop[k, 1] = go(sums.at[k, :, theirs, half:width], first_y.at[k], y_peer)

    def second_x(k):
        hop[k, 0].wait_recv()
        total = sums[k, x, :, 0:half].astype(jnp.float32) + first_x[k].astype(jnp.float32)
        sums[k, x, :, 0:half] = total.astype(jnp.bfloat16)
        hop[k, 3] = go(sums.at[k, x, theirs, 0:half], second_in.at[k, 0], y_peer)

    def second_y(k):
        hop[k, 1].wait_recv()
        for xx in range(2):
            total = sums[k, xx, mine, half:width].astype(jnp.float32) + first_y[k, xx].astype(
                jnp.float32
            )
            sums[k, xx, mine, half:width] = total.astype(jnp.bfloat16)
        hop[k, 4] = go(sums.at[k, 1 - x, mine, half:width], second_in.at[k, 1], x_peer)

    home = {}

    def homeward(k):
        for piece_index in range(2):
            cols = slice(piece_index * half, (piece_index + 1) * half)
            hop[k, 3 + piece_index].wait_recv()
            total = sums[k, x, mine, cols].astype(jnp.float32) + second_in[
                k, piece_index
            ].astype(jnp.float32)
            if k < parts:
                fin[k, :, cols] = total.astype(jnp.bfloat16)
            else:
                sums[k, x, mine, cols] = total.astype(jnp.bfloat16)
        if k >= parts:
            peer = dev(planes[k // parts], y, x, c)
            home[k] = go(sums.at[k, x, mine, :], fin.at[k], peer, keep=True)

    settled = []

    def settle(k):
        if k >= parts:
            home[k].wait_recv()
        first = planes[k // parts] * cap + k % parts * part
        place = lax.broadcasted_iota(jnp.int32, (tokens, part), 1) + first
        choose = (slot_column[:, 0:part].astype(jnp.int32) == place).astype(jnp.float32)
        choose = choose.astype(jnp.bfloat16)
        settled.append(k)
        for j in range(width // 256):
            cols = slice(j * 256, (j + 1) * 256)
            value = jnp.dot(choose, fin[k, :, cols], preferred_element_type=jnp.float32)
            if len(settled) > 1:
                value += unpermuted[:, cols]
            if len(settled) == len(chunks):
                moe_ref[:, cols] = value.astype(jnp.bfloat16)
            else:
                unpermuted[:, cols] = value

    rows, channels = feats.shape
    tiles = rows // 128
    reach = WINDOW_MAX

    def tile_rows(i, start=0, count=128):
        return pl.ds(pl.multiple_of(i * 128 + start, 16), count)

    mixer_copies = []

    def square_sums():
        mixer_load.wait()
        for load in small_loads[3:]:
            load.wait()

        @pl.loop(0, tiles)
        def _(i):
            total = jnp.zeros((128, 128), jnp.float32)
            for q in range(channels // 128):
                value = feats[tile_rows(i), q * 128 : (q + 1) * 128].astype(jnp.float32)
                total += value * value
            squares[pl.ds(i, 1), :] = jnp.sum(total.T, axis=0, keepdims=True)

        for index, peer in enumerate((core_peer, x_peer, cross_peer)):
            mixer_copies.append(
                go(squares, squares_in.at[index], peer)
            )

    def normalize():
        for copy in mixer_copies:
            copy.wait_recv()
        total = squares[...] + squares_in[0] + (squares_in[1] + squares_in[2])
        factors[...] = lax.rsqrt(total / D + EPS)

        @pl.loop(0, tiles)
        def _(i):
            factor = jnp.broadcast_to(factors[pl.ds(i, 1), :], (128, 128)).T
            for q in range(channels // 128):
                cols = slice(q * 128, (q + 1) * 128)
                value = feats[tile_rows(i), cols].astype(jnp.float32) * factor * gain_ref[:, cols]
                normed[tile_rows(i, reach), cols] = value.astype(jnp.bfloat16)

        following = lax.rem(ep + 1, 2 * GROUPS)
        mixer_copies.append(
            go(
                normed.at[rows : rows + reach, :],
                normed.at[0:reach, :],
                (following, tp),
                keep=True,
            )
        )

    def halo():
        mixer_copies[3].wait_recv()
        edge = normed[0:reach, :]
        normed[0:reach, :] = jnp.where(ep == 0, jnp.zeros_like(edge), edge)
        pool_load.wait()

    def pool(first, last):
        span = jnp.where(tp == 0, 2, jnp.where(tp == 1, 4, jnp.where(tp == 2, 8, 16)))

        @pl.loop(first, last)
        def _(i):
            position = ep * rows + i * 128 + lax.broadcasted_iota(jnp.int32, (128, 256), 0)
            share_of = 1.0 / jnp.minimum(position + 1, span).astype(jnp.float32)
            for q in range(channels // 256):
                cols = slice(q * 256, (q + 1) * 256)
                value = normed[tile_rows(i, 0, 128 + reach), cols].astype(jnp.float32)
                two = value + pltpu.roll(value, 1, 0)
                four = two + pltpu.roll(two, 2, 0)
                eight = four + pltpu.roll(four, 4, 0)
                sixteen = eight + pltpu.roll(eight, 8, 0)
                window = jnp.where(
                    tp == 0, two, jnp.where(tp == 1, four, jnp.where(tp == 2, eight, sixteen))
                )
                pooled = window[reach:] * share_of - value[reach:]
                feats[tile_rows(i), cols] = pooled.astype(jnp.bfloat16)
            projected = jnp.dot(
                feats[tile_rows(i), :], w_pool[...], preferred_element_type=jnp.float32
            )
            mixed_ref[tile_rows(i), :] = (projected * scale_ref[...]).astype(jnp.bfloat16)

    relay(0)
    arrive(2)
    diagonal(0)
    relay(1)
    arrive(5)
    relay(2)
    weights_ready()
    expand(0)
    relay(5)
    arrive(3)
    project(0)
    across(2)
    diagonal(1)
    diagonal(2)
    arrive(4)
    square_sums()
    arrive(6)
    expand(2)
    across(5)
    across(3)
    project(2)
    arrive(7)
    relay(4)
    across(6)
    diagonal(5)
    relay(3)
    expand(5)
    second_x(2)
    normalize()
    second_x(0)
    across(4)
    across(7)
    relay(6)
    diagonal(4)
    relay(7)
    second_y(0)
    second_y(2)
    project(5)
    halo()
    diagonal(6)
    expand(4)
    pool(0, 1)
    homeward(0)
    expand(1)
    project(4)
    diagonal(7)
    expand(7)
    second_x(5)
    second_y(5)
    expand(6)
    homeward(2)
    project(7)
    second_x(4)
    diagonal(3)
    pool(1, 2)
    second_y(4)
    project(6)
    expand(3)
    homeward(5)
    pool(2, 3)
    pool(3, 4)
    homeward(4)
    project(3)
    second_y(7)
    second_x(7)
    second_y(6)
    second_x(6)
    second_x(3)
    second_y(3)
    project(1)
    pool(4, 5)
    homeward(6)
    pool(5, 6)
    settle(0)
    homeward(7)
    pool(6, 7)
    settle(4)
    homeward(3)
    settle(2)
    second_x(1)
    second_y(1)
    pool(7, 8)
    settle(6)
    homeward(1)
    settle(5)
    settle(1)
    settle(3)
    settle(7)
    for index in kept + ring[-spare:]:
        started[index].wait_send()


def deliver(moe_in_ref, mixed_in_ref, moe_hbm, mixer_hbm, sem):
    copies = []
    for source, target, count in ((mixed_in_ref, mixer_hbm, 16), (moe_in_ref, moe_hbm, 4)):
        rows = source.shape[0] // count
        for i in range(count):
            at = slice(i * rows, (i + 1) * rows)
            copies.append(
                pltpu.make_async_copy(source.at[at], target.at[at], sem.at[len(copies)])
            )
    for copy in copies:
        copy.start()
    for copy in copies:
        copy.wait()


def paired_step(
    mixer_in,
    mixer_gain,
    pool_weight,
    pool_scale,
    moe_in,
    moe_gain,
    route_expert,
    route_weight,
    gate_weight,
    up_weight,
    down_weight,
):
    tokens, model = moe_in.shape
    n_ep, n_tp = lax.axis_size("ep"), lax.axis_size("tp")
    cap = 3 * tokens // n_ep
    width = model // n_tp
    units = gate_weight.shape[2]
    vmem = pl.BlockSpec(memory_space=pltpu.VMEM)
    hbm = pl.BlockSpec(memory_space=pl.ANY)
    dma = pltpu.SemaphoreType.DMA
    rows, channels = mixer_in.shape
    spare = 32
    copies, kept = 117, 22
    parts = 2
    chunks, part = GROUPS * parts, cap // parts
    moe_shape = (tokens, width)
    mixer_shape = (rows, channels)
    moe_out, mixed = pl.pallas_call(
        functools.partial(expert_kernel, cap, parts, spare),
        out_shape=(
            pltpu.VMEM(moe_shape, jnp.bfloat16),
            pltpu.VMEM(mixer_shape, jnp.bfloat16),
        ),
        in_specs=[hbm] * 11,
        out_specs=(vmem, vmem),
        scratch_shapes=[
            pltpu.VMEM((1, model), jnp.float32),
            pltpu.VMEM(route_expert.shape[::-1], jnp.int32),
            pltpu.VMEM(route_weight.shape[::-1], jnp.float32),
            pltpu.VMEM((1, channels), jnp.float32),
            pltpu.VMEM((1, channels), jnp.float32),
            pltpu.VMEM((tokens, model), jnp.bfloat16),
            pltpu.VMEM((tokens, 128), jnp.float32),
            pltpu.VMEM((tokens, width), jnp.bfloat16),
            pltpu.VMEM((6, cap, width), jnp.bfloat16),
            pltpu.VMEM((tokens, 128), jnp.float32),
            pltpu.VMEM((tokens, width), jnp.float32),
            pltpu.VMEM((n_tp, chunks, 2 * part, width), jnp.bfloat16),
            pltpu.VMEM((GROUPS, 8, 128), jnp.float32),
            pltpu.VMEM((n_ep, 8, 128), jnp.float32),
            pltpu.VMEM((n_ep * cap, 128), jnp.float32),
            pltpu.VMEM((n_ep * cap, 128), jnp.float32),
            pltpu.VMEM((model, units), jnp.bfloat16),
            pltpu.VMEM((model, units), jnp.bfloat16),
            pltpu.VMEM((2, 2 * units, width), jnp.bfloat16),
            pltpu.VMEM((2, chunks, 2 * part, units), jnp.bfloat16),
            pltpu.VMEM((chunks, 2, 2 * part, width), jnp.bfloat16),
            pltpu.VMEM((chunks, 2 * part, width // 2), jnp.bfloat16),
            pltpu.VMEM((chunks, 2, part, width // 2), jnp.bfloat16),
            pltpu.VMEM((chunks, 2, part, width // 2), jnp.bfloat16),
            pltpu.VMEM((chunks, part, width), jnp.bfloat16),
            dma((21,)),
            dma((spare + kept,)),
            dma((copies,)),
            pltpu.VMEM((rows, channels), jnp.bfloat16),
            pltpu.VMEM(pool_weight.shape[1:], jnp.bfloat16),
            pltpu.VMEM((rows // 128, 128), jnp.float32),
            pltpu.VMEM((3, rows // 128, 128), jnp.float32),
            pltpu.VMEM((rows // 128, 128), jnp.float32),
            pltpu.VMEM((rows + WINDOW_MAX, channels), jnp.bfloat16),
        ],
        compiler_params=pltpu.CompilerParams(
            collective_id=0, has_side_effects=True, vmem_limit_bytes=56 * 1024 * 1024
        ),
    )(
        moe_in,
        moe_gain[None, :],
        route_expert.T,
        route_weight.T,
        gate_weight[0],
        up_weight[0],
        down_weight[0],
        mixer_in,
        mixer_gain[None, :],
        pool_weight[0],
        pool_scale[None, :],
    )
    moe_out, mixer_out = pl.pallas_call(
        deliver,
        out_shape=(
            jax.ShapeDtypeStruct(moe_shape, jnp.bfloat16),
            jax.ShapeDtypeStruct(mixer_shape, jnp.bfloat16),
        ),
        in_specs=[vmem, vmem],
        out_specs=(hbm, hbm),
        scratch_shapes=[dma((20,))],
    )(
        pltpu.with_memory_space_constraint(moe_out, pltpu.VMEM),
        pltpu.with_memory_space_constraint(mixed, pltpu.VMEM),
    )
    return (mixer_out, moe_out)


def any_experts(
    moe_in, moe_gain, route_expert, route_weight, gate_weight, up_weight, down_weight
):
    tokens = moe_in.shape[0]
    feats_b = moe_in.astype(jnp.float32)
    normed_b = (
        feats_b * lax.rsqrt(jnp.mean(feats_b * feats_b, axis=1, keepdims=True) + EPS) * moe_gain
    ).astype(jnp.bfloat16)
    experts = gate_weight.shape[0] * lax.axis_size("ep")
    slots = 3 * tokens // experts
    flat = route_expert.reshape(-1)
    onehot = (flat[:, None] == jnp.arange(experts, dtype=jnp.int32)[None, :]).astype(jnp.int32)
    earlier = jnp.cumsum(onehot, axis=0) - onehot
    slot_index = flat * slots + jnp.sum(earlier * onehot, axis=1)
    owner = jnp.arange(2 * tokens, dtype=jnp.int32) // 2
    source = jnp.full((experts * slots,), tokens, jnp.int32).at[slot_index].set(owner)
    padded_b = jnp.concatenate([normed_b, jnp.zeros((1, D), jnp.bfloat16)], axis=0)
    outgoing = jnp.take(padded_b, source, axis=0).reshape(experts, slots, D)
    w_gate = gate_weight[0]
    w_up = up_weight[0]
    share = slots // lax.axis_size("tp")
    mine = lax.dynamic_slice_in_dim(outgoing, lax.axis_index("tp") * share, share, 1)
    arrived = lax.all_to_all(mine, "ep", split_axis=0, concat_axis=0, tiled=True)
    expand_arrived = lax.all_gather(arrived, "tp", axis=1, tiled=True)
    gate = jnp.einsum("nkd,df->nkf", expand_arrived, w_gate, preferred_element_type=jnp.float32)
    upper = jnp.einsum("nkd,df->nkf", expand_arrived, w_up, preferred_element_type=jnp.float32)
    hidden = (jax.nn.silu(gate) * upper).astype(jnp.bfloat16)
    flat_hidden = hidden.reshape(-1, hidden.shape[2])
    w_down = down_weight[0]
    columns = D // lax.axis_size("tp")
    summed = lax.psum_scatter(
        lax.dot_general(
            w_down, flat_hidden, (((0,), (1,)), ((), ())), preferred_element_type=jnp.float32
        ),
        "tp",
        scatter_dimension=0,
        tiled=True,
    ).astype(jnp.bfloat16)
    back = lax.all_to_all(
        summed.reshape(columns, -1, slots), "ep", split_axis=1, concat_axis=1, tiled=True
    )
    picked = jnp.take(back.reshape(columns, experts * slots), slot_index, axis=1)
    weighted = picked.astype(jnp.float32).reshape(columns, tokens, 2) * route_weight[None, :, :]
    moe_out = jnp.sum(weighted, axis=2).T.astype(jnp.bfloat16)
    return moe_out


def general_step(
    mixer_in,
    mixer_gain,
    pool_weight,
    pool_scale,
    moe_in,
    moe_gain,
    route_expert,
    route_weight,
    gate_weight,
    up_weight,
    down_weight,
):
    rows = mixer_in.shape[0]
    feats = mixer_in.astype(jnp.float32)
    squares = lax.psum(jnp.sum(feats * feats, axis=1), "tp")
    normed_a = (feats * lax.rsqrt(squares[:, None] / D + EPS) * mixer_gain).astype(jnp.bfloat16)
    reach = WINDOW_MAX - 1
    before = passed_along(normed_a[rows - reach :], "ep", 1)
    extended = jnp.concatenate([before, normed_a], axis=0).astype(jnp.float32)
    running = jnp.zeros((rows, normed_a.shape[1]), jnp.float32)
    totals = []
    for offset in range(WINDOW_MAX):
        running = running + lax.slice_in_dim(
            extended, reach - offset, reach - offset + rows, axis=0
        )
        if offset > 0 and offset + 1 & offset == 0:
            totals.append(running)
    group = lax.axis_index("tp")
    window_sum = lax.dynamic_index_in_dim(jnp.stack(totals), group, 0, keepdims=False)
    span = jnp.left_shift(jnp.int32(2), group)
    position = lax.axis_index("ep") * rows + jnp.arange(rows, dtype=jnp.int32)
    count = jnp.minimum(position + 1, span).astype(jnp.float32)[:, None]
    pooled = (window_sum / count - extended[reach:]).astype(jnp.bfloat16)
    mixer_out = (
        jnp.dot(pooled, pool_weight[0], preferred_element_type=jnp.float32) * pool_scale
    ).astype(jnp.bfloat16)
    moe_out = any_experts(
        moe_in, moe_gain, route_expert, route_weight, gate_weight, up_weight, down_weight
    )
    return (mixer_out, moe_out)


def solution(mesh):
    paired = mesh.shape["ep"] == 2 * GROUPS and mesh.shape["tp"] == 4
    return jax.shard_map(
        paired_step if paired else general_step,
        mesh=mesh,
        in_specs=(
            P("ep", "tp"),
            P("tp"),
            P("tp", None, None),
            P("tp"),
            P("ep", None),
            P(),
            P("ep", None),
            P("ep", None),
            P("ep", None, "tp"),
            P("ep", None, "tp"),
            P("ep", "tp", None),
        ),
        out_specs=(P("ep", "tp"), P("ep", "tp")),
        check_vma=False,
    )
```

```python
import functools

import jax
import jax.numpy as jnp
from jax import lax
from jax.experimental import pallas as pl
from jax.experimental.pallas import tpu as pltpu
from jax.sharding import PartitionSpec as P

D = 4096
WINDOW_MAX = 16


EPS = 1e-06


def passed_along(value, axis, steps):
    count = lax.axis_size(axis)
    first, last = (max(0, -steps), min(count, count - steps))
    return lax.ppermute(value, axis, [(source, source + steps) for source in range(first, last)])


GROUPS = 4
MESH = pl.DeviceIdType.MESH


def expert_kernel(
    cap,
    parts,
    spare,
    moe_hbm,
    moe_gain_hbm,
    routes_hbm,
    shares_hbm,
    gate_hbm,
    up_hbm,
    down_hbm,
    mixer_hbm,
    gain_hbm,
    pool_hbm,
    scale_hbm,
    moe_ref,
    mixed_ref,
    moe_gain_ref,
    routes_ref,
    shares_ref,
    gain_ref,
    scale_ref,
    tokens_in,
    row_factor,
    scaled,
    outgoing,
    slot_column,
    unpermuted,
    xbuf,
    wrow,
    wbuf,
    wcol,
    fcol,
    w_gate,
    w_up,
    w_down,
    hidden,
    sums,
    first_x,
    first_y,
    second_in,
    fin,
    local_sem,
    send_sem,
    recv_sem,
    feats,
    w_pool,
    squares,
    squares_in,
    factors,
    normed,
):
    ep, tp = lax.axis_index("ep"), lax.axis_index("tp")
    z, y = ep // 2, ep % 2
    x, c = tp // 2, tp % 2
    tokens, model = tokens_in.shape
    width = xbuf.shape[3]
    units = w_gate.shape[1]
    half = width // 2
    part = cap // parts
    pair = 2 * part
    mine, theirs = slice(0, part), slice(part, pair)
    chunks = range(GROUPS * parts)
    eighth = width // 8
    direct = tuple(share * eighth for share in (4, 4, 0, 0, 0, 0, 8, 8))

    def dev(zz, yy, xx, cc):
        return (zz * 2 + yy, xx * 2 + cc)

    planes = [z, z + 1 - 2 * (z % 2), lax.rem(z + 2, GROUPS), GROUPS - 1 - z]
    core_peer = dev(z, y, x, 1 - c)
    x_peer = dev(z, y, 1 - x, c)
    y_peer = dev(z, 1 - y, x, c)
    cross_peer = dev(z, y, 1 - x, 1 - c)
    xq = (1 - x) * 2 + c

    def columns(quarter, count=None, offset=0):
        start = pl.multiple_of(quarter * width + offset, 128)
        return pl.ds(start, width if count is None else count)

    quarters = (tp, xq, x * 2 + 1 - c, (1 - x) * 2 + 1 - c)
    rows_half = tokens // 2
    small_loads = [
        pltpu.make_async_copy(source, target, local_sem.at[16 + i])
        for i, (source, target) in enumerate(
            (
                (routes_hbm, routes_ref),
                (shares_hbm, shares_ref),
                (moe_gain_hbm, moe_gain_ref),
                (gain_hbm, gain_ref),
                (scale_hbm, scale_ref),
            )
        )
    ]
    token_loads = []
    for i, quarter in enumerate(quarters):
        for b in range(2):
            at = (slice(b * rows_half, (b + 1) * rows_half), columns(quarter))
            token_loads.append(
                pltpu.make_async_copy(
                    moe_hbm.at[at], tokens_in.at[at], local_sem.at[i * 2 + b]
                )
            )
    mixer_load = pltpu.make_async_copy(mixer_hbm, feats, local_sem.at[8])
    pool_load = pltpu.make_async_copy(pool_hbm, w_pool, local_sem.at[9])
    loads = [
        pltpu.make_async_copy(gate_hbm, w_gate, local_sem.at[10]),
        pltpu.make_async_copy(up_hbm, w_up, local_sem.at[11]),
    ]
    down_rows = pl.ds(pl.multiple_of(c * units, units), units)
    for xx in range(2):
        loads.append(
            pltpu.make_async_copy(
                down_hbm.at[:, columns(xx * 2 + c)],
                w_down.at[xx, down_rows, :],
                local_sem.at[12 + xx],
            )
        )
    for load in small_loads[:3] + token_loads + small_loads[3:]:
        load.start()

    barrier = pltpu.get_barrier_semaphore()
    peers = [core_peer, x_peer, y_peer, cross_peer]
    for other in range(2):
        for k in range(1, GROUPS):
            peers.append(dev(planes[k], lax.rem(y + other, 2), x, c))
    for peer in peers:
        pl.semaphore_signal(barrier, inc=1, device_id=peer, device_id_type=MESH)

    started = []

    ring = []
    kept = []
    arrivals = [0]
    clock = [0]
    exchanged = {id(core_peer): [], id(x_peer): [], id(y_peer): []}

    class Copy:
        def __init__(self, copy):
            self.copy, self.sent, self.waited = copy, clock[0], None
            self.wait_send = copy.wait_send

        def wait_recv(self):
            self.copy.wait_recv()
            clock[0] += 1
            self.waited = clock[0]

    def receiver(past):
        heard = max((copy.sent for copy in past if copy.waited is not None), default=0)
        latest = {copy.index: copy for copy in past}
        for index, copy in latest.items():
            if copy.waited is not None and copy.waited < heard:
                return index
        arrivals[0] += 1
        return arrivals[0] - 1

    def go(src, dst, peer, keep=False):
        index = len(started)
        if keep:
            send = spare + len(kept)
            kept.append(index)
        else:
            send = len(ring) % spare
            if len(ring) >= spare:
                started[ring[-spare]].wait_send()
            ring.append(index)
        past = exchanged.get(id(peer), [])
        receive = receiver(past)
        copy = pltpu.make_async_remote_copy(
            src_ref=src,
            dst_ref=dst,
            send_sem=send_sem.at[send],
            recv_sem=recv_sem.at[receive],
            device_id=peer,
            device_id_type=MESH,
        )
        copy.start()
        clock[0] += 1
        started.append(Copy(copy))
        started[-1].index = receive
        past.append(started[-1])
        return started[-1]

    for load in small_loads[:3]:
        load.wait()
    routes = routes_ref[...]
    group = jnp.right_shift(routes[0:1, :], 1)
    lane_group = lax.broadcasted_iota(jnp.int32, (8, tokens), 0)
    member = lane_group == group
    earlier = lax.broadcasted_iota(jnp.int32, (tokens, tokens), 0) < lax.broadcasted_iota(
        jnp.int32, (tokens, tokens), 1
    )
    ahead = jnp.dot(
        member.astype(jnp.bfloat16), earlier.astype(jnp.bfloat16), preferred_element_type=jnp.float32
    )
    rank = jnp.sum(jnp.where(member, ahead, 0.0), axis=0, keepdims=True).astype(jnp.int32)

    def picks(k, count):
        place = lax.broadcasted_iota(jnp.int32, (count, tokens), 0)
        return (place == rank) & (group == planes[k])

    parity = jnp.bitwise_and(routes, 1)
    shares = shares_ref[...]
    by_expert = jnp.sum(
        jnp.concatenate(
            [
                jnp.where(lane_group == parity[r : r + 1, :], shares[r : r + 1, :], 0.0)[None]
                for r in range(2)
            ],
            axis=0,
        ),
        axis=0,
    )
    slot = (group * cap + rank).astype(jnp.float32)
    for b in range(tokens // 128):
        row = slot[:, b * 128 : (b + 1) * 128]
        slot_column[b * 128 : (b + 1) * 128, :] = jnp.broadcast_to(row, (128, 128)).T

    def send_lines():
        for b in range(8):
            rows = slice(b * tokens // 8, (b + 1) * tokens // 8)
            total = jnp.zeros((tokens // 8, 128), jnp.float32)
            for q in range(model // 128):
                value = tokens_in[rows, q * 128 : (q + 1) * 128].astype(jnp.float32)
                total += value * value
            mean = jnp.sum(total, axis=1, keepdims=True) / D
            row_factor[rows, :] = jnp.broadcast_to(lax.rsqrt(mean + EPS), (tokens // 8, 128))
        factor = jnp.concatenate(
            [row_factor[b * 128 : (b + 1) * 128, :].T[0:8, :] for b in range(tokens // 128)], axis=1
        )
        lines = jnp.where(lane_group == 2, factor, by_expert)
        copies = []
        for k in range(GROUPS):
            wrow[k] = lax.dot_general(
                lines,
                picks(k, 128).astype(jnp.float32),
                (((1,), (1,)), ((), ())),
                precision=lax.Precision.HIGHEST,
                preferred_element_type=jnp.float32,
            )
            for r in range(2):
                if k or r:
                    peer = dev(planes[k], lax.rem(y + r, 2), x, c)
                    copies.append(go(wrow.at[k], wbuf.at[k * 2 + r], peer))
        wbuf[0] = wrow[0]
        return copies

    for load in token_loads[:2]:
        load.wait()
    for load in (mixer_load, *loads, pool_load):
        load.start()

    def scale_quarter(quarter):
        for j in range(width // 128):
            cols = columns(quarter, 128, j * 128)
            value = tokens_in[:, cols].astype(jnp.float32) * moe_gain_ref[:, cols]
            scaled[:, j * 128 : (j + 1) * 128] = value.astype(jnp.bfloat16)

    def own_rows(quarter):
        return [xbuf.at[quarter, h, mine] for h in range(parts)]

    def pick_rows(quarter, groups, targets):
        scale_quarter(quarter)
        choose = jnp.concatenate(
            [picks(k, cap).astype(jnp.float32) for k in groups], axis=0
        ).astype(jnp.bfloat16)
        for j in range(width // 256):
            cols = slice(j * 256, (j + 1) * 256)
            picked = jnp.dot(
                choose, scaled[:, cols], preferred_element_type=jnp.float32
            ).astype(jnp.bfloat16)
            start = 0
            for target in targets:
                target[:, cols] = picked[start : start + target.shape[0]]
                start += target.shape[0]

    zcopies = {}
    piece = {}

    def depart(k, across):
        g = k // parts
        index = g + 2 if across else g - 1
        rows = slice(k % parts * part, (k % parts + 1) * part)
        zcopies[k, across] = go(
            outgoing.at[index, rows],
            xbuf.at[xq if across else tp, k, mine],
            dev(planes[g], y, x, c),
            keep=True,
        )

    def share(name, k, quarter, source, target, peer, start=0, stop=None):
        stop = width if stop is None else stop
        if start < stop:
            cols = pl.ds(start, stop - start)
            piece[name, k] = go(
                xbuf.at[quarter, k, source, cols], xbuf.at[quarter, k, target, cols], peer
            )

    pick_rows(tp, (1, 2, 3, 0), [outgoing.at[i] for i in range(3)] + own_rows(tp))
    pl.semaphore_wait(barrier, len(peers))
    depart(5, 0)
    for k in range(parts):
        share("y", k, tp, mine, theirs, y_peer)
    for load in token_loads[2:]:
        load.wait()
    wcopies = send_lines()
    pick_rows(xq, (1, 0), [outgoing.at[3]] + own_rows(xq))
    depart(2, 0)
    depart(3, 0)
    depart(2, 1)
    depart(6, 0)
    depart(4, 0)
    depart(7, 0)
    depart(3, 1)
    for k in range(parts):
        share("d0", k, xq, mine, theirs, y_peer, 0, direct[k])
    down_copies = []
    for xx in range(2):
        down_copies.append(
            go(down_hbm.at[:, columns(xx * 2 + 1 - c)], w_down.at[xx, down_rows, :], core_peer)
        )
    for quarter in quarters[2:]:
        pick_rows(quarter, (0,), own_rows(quarter))

    def arrive(k):
        zcopies[k, 0].wait_recv()
        share("y", k, tp, mine, theirs, y_peer)
        if (k, 1) not in zcopies:
            share("x", k, tp, mine, mine, x_peer)
        share("c", k, tp, mine, mine, core_peer)

    def across(k):
        if (k, 1) in zcopies:
            zcopies[k, 1].wait_recv()
        else:
            piece["x", k].wait_recv()
        share("d0", k, xq, mine, theirs, y_peer, 0, direct[k])
        share("xc", k, xq, mine, mine, core_peer)

    def relay(k):
        piece["y", k].wait_recv()
        share("d1", k, tp, theirs, theirs, x_peer, direct[k])
        share("yc", k, tp, theirs, theirs, core_peer)

    def diagonal(k):
        for name in ("d0", "d1"):
            if (name, k) in piece:
                piece[name, k].wait_recv()
        share("dc", k, xq, theirs, theirs, core_peer)

    def complete(k):
        for name in ("c", "xc", "yc", "dc"):
            if (name, k) in piece:
                piece[name, k].wait_recv()

    hidden_away = {}

    def weights_ready():
        for copy in wcopies:
            copy.wait_recv()
        for source in range(wbuf.shape[0]):
            line = jnp.where(y == 0, wbuf[source, 0:1, :], wbuf[source, 1:2, :])
            at = slice(source * cap, (source + 1) * cap)
            wcol[at, :] = jnp.broadcast_to(line, (128, 128)).T[:cap]
            fcol[at, :] = jnp.broadcast_to(wbuf[source, 2:3, :], (128, 128)).T[:cap]
        for load in loads:
            load.wait()
        for copy in down_copies:
            copy.wait_recv()

    def expand(k):
        complete(k)
        gate = jnp.zeros((pair, units), jnp.float32)
        upper = gate
        for q in range(xbuf.shape[0]):
            rows = xbuf[q, k]
            gate += jnp.dot(
                rows, w_gate[q * width : (q + 1) * width, :], preferred_element_type=jnp.float32
            )
            upper += jnp.dot(
                rows, w_up[q * width : (q + 1) * width, :], preferred_element_type=jnp.float32
            )
        first = k // parts * 2 * cap + k % parts * part

        def spread(table):
            lines = [table[first : first + part, :], table[first + cap : first + cap + part, :]]
            return jnp.concatenate([jnp.concatenate(lines, axis=0)] * (units // 128), axis=1)

        factor = spread(fcol)
        gate, upper = gate * factor, upper * factor
        value = (gate / (1.0 + jnp.exp(-gate))) * upper * spread(wcol)
        hidden[c, k] = value.astype(jnp.bfloat16)
        hidden_away[k] = go(hidden.at[c, k], hidden.at[c, k], core_peer)

    hop = {}

    def project(k):
        hidden_away[k].wait_recv()
        for xx in range(2):
            for j in range(2):
                cols = slice(j * half, (j + 1) * half)
                total = jnp.dot(
                    hidden[0, k], w_down[xx, 0:units, cols], preferred_element_type=jnp.float32
                ) + jnp.dot(
                    hidden[1, k], w_down[xx, units:, cols], preferred_element_type=jnp.float32
                )
                sums[k, xx, :, cols] = total.astype(jnp.bfloat16)
        hop[k, 0] = go(sums.at[k, 1 - x, :, 0:half], first_x.at[k], x_peer)
        hop[k, 1] = go(sums.at[k, :, theirs, half:width], first_y.at[k], y_peer)

    def second_x(k):
        hop[k, 0].wait_recv()
        total = sums[k, x, :, 0:half].astype(jnp.float32) + first_x[k].astype(jnp.float32)
        sums[k, x, :, 0:half] = total.astype(jnp.bfloat16)
        hop[k, 3] = go(sums.at[k, x, theirs, 0:half], second_in.at[k, 0], y_peer)

    def second_y(k):
        hop[k, 1].wait_recv()
        for xx in range(2):
            total = sums[k, xx, mine, half:width].astype(jnp.float32) + first_y[k, xx].astype(
                jnp.float32
            )
            sums[k, xx, mine, half:width] = total.astype(jnp.bfloat16)
        hop[k, 4] = go(sums.at[k, 1 - x, mine, half:width], second_in.at[k, 1], x_peer)

    home = {}

    def homeward(k):
        for piece_index in range(2):
            cols = slice(piece_index * half, (piece_index + 1) * half)
            hop[k, 3 + piece_index].wait_recv()
            total = sums[k, x, mine, cols].astype(jnp.float32) + second_in[
                k, piece_index
            ].astype(jnp.float32)
            if k < parts:
                fin[k, :, cols] = total.astype(jnp.bfloat16)
            else:
                sums[k, x, mine, cols] = total.astype(jnp.bfloat16)
        if k >= parts:
            peer = dev(planes[k // parts], y, x, c)
            home[k] = go(sums.at[k, x, mine, :], fin.at[k], peer)

    settled = []

    def settle(k):
        if k >= parts:
            home[k].wait_recv()
        first = planes[k // parts] * cap + k % parts * part
        place = lax.broadcasted_iota(jnp.int32, (tokens, part), 1) + first
        choose = (slot_column[:, 0:part].astype(jnp.int32) == place).astype(jnp.float32)
        choose = choose.astype(jnp.bfloat16)
        settled.append(k)
        for j in range(width // 256):
            cols = slice(j * 256, (j + 1) * 256)
            value = jnp.dot(choose, fin[k, :, cols], preferred_element_type=jnp.float32)
            if len(settled) > 1:
                value += unpermuted[:, cols]
            if len(settled) == len(chunks):
                moe_ref[:, cols] = value.astype(jnp.bfloat16)
            else:
                unpermuted[:, cols] = value

    rows, channels = feats.shape
    tiles = rows // 128
    reach = WINDOW_MAX

    def tile_rows(i, start=0, count=128):
        return pl.ds(pl.multiple_of(i * 128 + start, 16), count)

    mixer_copies = []

    def square_sums():
        mixer_load.wait()
        for load in small_loads[3:]:
            load.wait()

        @pl.loop(0, tiles)
        def _(i):
            total = jnp.zeros((128, 128), jnp.float32)
            for q in range(channels // 128):
                value = feats[tile_rows(i), q * 128 : (q + 1) * 128].astype(jnp.float32)
                total += value * value
            squares[pl.ds(i, 1), :] = jnp.sum(total.T, axis=0, keepdims=True)

        for index, peer in enumerate((core_peer, x_peer, cross_peer)):
            mixer_copies.append(
                go(squares, squares_in.at[index], peer)
            )

    def normalize():
        for copy in mixer_copies:
            copy.wait_recv()
        total = squares[...] + squares_in[0] + (squares_in[1] + squares_in[2])
        factors[...] = lax.rsqrt(total / D + EPS)

        @pl.loop(0, tiles)
        def _(i):
            factor = jnp.broadcast_to(factors[pl.ds(i, 1), :], (128, 128)).T
            for q in range(channels // 128):
                cols = slice(q * 128, (q + 1) * 128)
                value = feats[tile_rows(i), cols].astype(jnp.float32) * factor * gain_ref[:, cols]
                normed[tile_rows(i, reach), cols] = value.astype(jnp.bfloat16)

        following = lax.rem(ep + 1, 2 * GROUPS)
        mixer_copies.append(
            go(
                normed.at[rows : rows + reach, :],
                normed.at[0:reach, :],
                (following, tp),
            )
        )

    def halo():
        mixer_copies[3].wait_recv()
        edge = normed[0:reach, :]
        normed[0:reach, :] = jnp.where(ep == 0, jnp.zeros_like(edge), edge)
        pool_load.wait()

    def pool(first, last):
        span = jnp.where(tp == 0, 2, jnp.where(tp == 1, 4, jnp.where(tp == 2, 8, 16)))

        @pl.loop(first, last)
        def _(i):
            position = ep * rows + i * 128 + lax.broadcasted_iota(jnp.int32, (128, 256), 0)
            share_of = 1.0 / jnp.minimum(position + 1, span).astype(jnp.float32)
            for q in range(channels // 256):
                cols = slice(q * 256, (q + 1) * 256)
                value = normed[tile_rows(i, 0, 128 + reach), cols].astype(jnp.float32)
                two = value + pltpu.roll(value, 1, 0)
                four = two + pltpu.roll(two, 2, 0)
                eight = four + pltpu.roll(four, 4, 0)
                sixteen = eight + pltpu.roll(eight, 8, 0)
                window = jnp.where(
                    tp == 0, two, jnp.where(tp == 1, four, jnp.where(tp == 2, eight, sixteen))
                )
                pooled = window[reach:] * share_of - value[reach:]
                feats[tile_rows(i), cols] = pooled.astype(jnp.bfloat16)
            projected = jnp.dot(
                feats[tile_rows(i), :], w_pool[...], preferred_element_type=jnp.float32
            )
            mixed_ref[tile_rows(i), :] = (projected * scale_ref[...]).astype(jnp.bfloat16)

    relay(0)
    arrive(2)
    diagonal(0)
    relay(1)
    arrive(5)
    relay(2)
    weights_ready()
    expand(0)
    relay(5)
    arrive(3)
    project(0)
    across(2)
    diagonal(1)
    diagonal(2)
    arrive(4)
    square_sums()
    arrive(6)
    expand(2)
    across(5)
    across(3)
    project(2)
    arrive(7)
    relay(4)
    across(6)
    diagonal(5)
    relay(3)
    expand(5)
    second_x(2)
    normalize()
    second_x(0)
    across(4)
    across(7)
    relay(6)
    diagonal(4)
    relay(7)
    second_y(0)
    second_y(2)
    project(5)
    diagonal(6)
    expand(4)
    halo()
    pool(0, 1)
    homeward(0)
    expand(1)
    project(4)
    diagonal(7)
    expand(7)
    second_x(5)
    second_y(5)
    expand(6)
    homeward(2)
    project(7)
    second_x(4)
    diagonal(3)
    pool(1, 2)
    second_y(4)
    project(6)
    expand(3)
    homeward(5)
    pool(2, 3)
    pool(3, 4)
    homeward(4)
    project(3)
    second_y(7)
    second_x(7)
    second_y(6)
    second_x(6)
    second_x(3)
    second_y(3)
    project(1)
    pool(4, 5)
    homeward(6)
    pool(5, 6)
    settle(0)
    homeward(7)
    pool(6, 7)
    settle(4)
    homeward(3)
    settle(2)
    second_x(1)
    second_y(1)
    pool(7, 8)
    settle(6)
    homeward(1)
    settle(5)
    settle(1)
    settle(3)
    settle(7)
    for index in kept + ring[-spare:]:
        started[index].wait_send()


def deliver(moe_in_ref, mixed_in_ref, moe_hbm, mixer_hbm, sem):
    copies = []
    for source, target, count in ((mixed_in_ref, mixer_hbm, 16), (moe_in_ref, moe_hbm, 4)):
        rows = source.shape[0] // count
        for i in range(count):
            at = slice(i * rows, (i + 1) * rows)
            copies.append(
                pltpu.make_async_copy(source.at[at], target.at[at], sem.at[len(copies)])
            )
    for copy in copies:
        copy.start()
    for copy in copies:
        copy.wait()


def paired_step(
    mixer_in,
    mixer_gain,
    pool_weight,
    pool_scale,
    moe_in,
    moe_gain,
    route_expert,
    route_weight,
    gate_weight,
    up_weight,
    down_weight,
):
    tokens, model = moe_in.shape
    n_ep, n_tp = lax.axis_size("ep"), lax.axis_size("tp")
    cap = 3 * tokens // n_ep
    width = model // n_tp
    units = gate_weight.shape[2]
    vmem = pl.BlockSpec(memory_space=pltpu.VMEM)
    hbm = pl.BlockSpec(memory_space=pl.ANY)
    dma = pltpu.SemaphoreType.DMA
    rows, channels = mixer_in.shape
    spare = 32
    copies, kept = 67, 8
    parts = 2
    chunks, part = GROUPS * parts, cap // parts
    moe_shape = (tokens, width)
    mixer_shape = (rows, channels)
    moe_out, mixed = pl.pallas_call(
        functools.partial(expert_kernel, cap, parts, spare),
        out_shape=(
            pltpu.VMEM(moe_shape, jnp.bfloat16),
            pltpu.VMEM(mixer_shape, jnp.bfloat16),
        ),
        in_specs=[hbm] * 11,
        out_specs=(vmem, vmem),
        scratch_shapes=[
            pltpu.VMEM((1, model), jnp.float32),
            pltpu.VMEM(route_expert.shape[::-1], jnp.int32),
            pltpu.VMEM(route_weight.shape[::-1], jnp.float32),
            pltpu.VMEM((1, channels), jnp.float32),
            pltpu.VMEM((1, channels), jnp.float32),
            pltpu.VMEM((tokens, model), jnp.bfloat16),
            pltpu.VMEM((tokens, 128), jnp.float32),
            pltpu.VMEM((tokens, width), jnp.bfloat16),
            pltpu.VMEM((6, cap, width), jnp.bfloat16),
            pltpu.VMEM((tokens, 128), jnp.float32),
            pltpu.VMEM((tokens, width), jnp.float32),
            pltpu.VMEM((n_tp, chunks, 2 * part, width), jnp.bfloat16),
            pltpu.VMEM((GROUPS, 8, 128), jnp.float32),
            pltpu.VMEM((n_ep, 8, 128), jnp.float32),
            pltpu.VMEM((n_ep * cap, 128), jnp.float32),
            pltpu.VMEM((n_ep * cap, 128), jnp.float32),
            pltpu.VMEM((model, units), jnp.bfloat16),
            pltpu.VMEM((model, units), jnp.bfloat16),
            pltpu.VMEM((2, 2 * units, width), jnp.bfloat16),
            pltpu.VMEM((2, chunks, 2 * part, units), jnp.bfloat16),
            pltpu.VMEM((chunks, 2, 2 * part, width), jnp.bfloat16),
            pltpu.VMEM((chunks, 2 * part, width // 2), jnp.bfloat16),
            pltpu.VMEM((chunks, 2, part, width // 2), jnp.bfloat16),
            pltpu.VMEM((chunks, 2, part, width // 2), jnp.bfloat16),
            pltpu.VMEM((chunks, part, width), jnp.bfloat16),
            dma((21,)),
            dma((spare + kept,)),
            dma((copies,)),
            pltpu.VMEM((rows, channels), jnp.bfloat16),
            pltpu.VMEM(pool_weight.shape[1:], jnp.bfloat16),
            pltpu.VMEM((rows // 128, 128), jnp.float32),
            pltpu.VMEM((3, rows // 128, 128), jnp.float32),
            pltpu.VMEM((rows // 128, 128), jnp.float32),
            pltpu.VMEM((rows + WINDOW_MAX, channels), jnp.bfloat16),
        ],
        compiler_params=pltpu.CompilerParams(
            collective_id=0, has_side_effects=True, vmem_limit_bytes=56 * 1024 * 1024
        ),
    )(
        moe_in,
        moe_gain[None, :],
        route_expert.T,
        route_weight.T,
        gate_weight[0],
        up_weight[0],
        down_weight[0],
        mixer_in,
        mixer_gain[None, :],
        pool_weight[0],
        pool_scale[None, :],
    )
    moe_out, mixer_out = pl.pallas_call(
        deliver,
        out_shape=(
            jax.ShapeDtypeStruct(moe_shape, jnp.bfloat16),
            jax.ShapeDtypeStruct(mixer_shape, jnp.bfloat16),
        ),
        in_specs=[vmem, vmem],
        out_specs=(hbm, hbm),
        scratch_shapes=[dma((20,))],
    )(
        pltpu.with_memory_space_constraint(moe_out, pltpu.VMEM),
        pltpu.with_memory_space_constraint(mixed, pltpu.VMEM),
    )
    return (mixer_out, moe_out)


def any_experts(
    moe_in, moe_gain, route_expert, route_weight, gate_weight, up_weight, down_weight
):
    tokens = moe_in.shape[0]
    feats_b = moe_in.astype(jnp.float32)
    normed_b = (
        feats_b * lax.rsqrt(jnp.mean(feats_b * feats_b, axis=1, keepdims=True) + EPS) * moe_gain
    ).astype(jnp.bfloat16)
    experts = gate_weight.shape[0] * lax.axis_size("ep")
    slots = 3 * tokens // experts
    flat = route_expert.reshape(-1)
    onehot = (flat[:, None] == jnp.arange(experts, dtype=jnp.int32)[None, :]).astype(jnp.int32)
    earlier = jnp.cumsum(onehot, axis=0) - onehot
    slot_index = flat * slots + jnp.sum(earlier * onehot, axis=1)
    owner = jnp.arange(2 * tokens, dtype=jnp.int32) // 2
    source = jnp.full((experts * slots,), tokens, jnp.int32).at[slot_index].set(owner)
    padded_b = jnp.concatenate([normed_b, jnp.zeros((1, D), jnp.bfloat16)], axis=0)
    outgoing = jnp.take(padded_b, source, axis=0).reshape(experts, slots, D)
    w_gate = gate_weight[0]
    w_up = up_weight[0]
    share = slots // lax.axis_size("tp")
    mine = lax.dynamic_slice_in_dim(outgoing, lax.axis_index("tp") * share, share, 1)
    arrived = lax.all_to_all(mine, "ep", split_axis=0, concat_axis=0, tiled=True)
    expand_arrived = lax.all_gather(arrived, "tp", axis=1, tiled=True)
    gate = jnp.einsum("nkd,df->nkf", expand_arrived, w_gate, preferred_element_type=jnp.float32)
    upper = jnp.einsum("nkd,df->nkf", expand_arrived, w_up, preferred_element_type=jnp.float32)
    hidden = (jax.nn.silu(gate) * upper).astype(jnp.bfloat16)
    flat_hidden = hidden.reshape(-1, hidden.shape[2])
    w_down = down_weight[0]
    columns = D // lax.axis_size("tp")
    summed = lax.psum_scatter(
        lax.dot_general(
            w_down, flat_hidden, (((0,), (1,)), ((), ())), preferred_element_type=jnp.float32
        ),
        "tp",
        scatter_dimension=0,
        tiled=True,
    ).astype(jnp.bfloat16)
    back = lax.all_to_all(
        summed.reshape(columns, -1, slots), "ep", split_axis=1, concat_axis=1, tiled=True
    )
    picked = jnp.take(back.reshape(columns, experts * slots), slot_index, axis=1)
    weighted = picked.astype(jnp.float32).reshape(columns, tokens, 2) * route_weight[None, :, :]
    moe_out = jnp.sum(weighted, axis=2).T.astype(jnp.bfloat16)
    return moe_out


def general_step(
    mixer_in,
    mixer_gain,
    pool_weight,
    pool_scale,
    moe_in,
    moe_gain,
    route_expert,
    route_weight,
    gate_weight,
    up_weight,
    down_weight,
):
    rows = mixer_in.shape[0]
    feats = mixer_in.astype(jnp.float32)
    squares = lax.psum(jnp.sum(feats * feats, axis=1), "tp")
    normed_a = (feats * lax.rsqrt(squares[:, None] / D + EPS) * mixer_gain).astype(jnp.bfloat16)
    reach = WINDOW_MAX - 1
    before = passed_along(normed_a[rows - reach :], "ep", 1)
    extended = jnp.concatenate([before, normed_a], axis=0).astype(jnp.float32)
    running = jnp.zeros((rows, normed_a.shape[1]), jnp.float32)
    totals = []
    for offset in range(WINDOW_MAX):
        running = running + lax.slice_in_dim(
            extended, reach - offset, reach - offset + rows, axis=0
        )
        if offset > 0 and offset + 1 & offset == 0:
            totals.append(running)
    group = lax.axis_index("tp")
    window_sum = lax.dynamic_index_in_dim(jnp.stack(totals), group, 0, keepdims=False)
    span = jnp.left_shift(jnp.int32(2), group)
    position = lax.axis_index("ep") * rows + jnp.arange(rows, dtype=jnp.int32)
    count = jnp.minimum(position + 1, span).astype(jnp.float32)[:, None]
    pooled = (window_sum / count - extended[reach:]).astype(jnp.bfloat16)
    mixer_out = (
        jnp.dot(pooled, pool_weight[0], preferred_element_type=jnp.float32) * pool_scale
    ).astype(jnp.bfloat16)
    moe_out = any_experts(
        moe_in, moe_gain, route_expert, route_weight, gate_weight, up_weight, down_weight
    )
    return (mixer_out, moe_out)


def solution(mesh):
    paired = mesh.shape["ep"] == 2 * GROUPS and mesh.shape["tp"] == 4
    return jax.shard_map(
        paired_step if paired else general_step,
        mesh=mesh,
        in_specs=(
            P("ep", "tp"),
            P("tp"),
            P("tp", None, None),
            P("tp"),
            P("ep", None),
            P(),
            P("ep", None),
            P("ep", None),
            P("ep", None, "tp"),
            P("ep", None, "tp"),
            P("ep", "tp", None),
        ),
        out_specs=(P("ep", "tp"), P("ep", "tp")),
        check_vma=False,
    )
```
